512 devices in a mesh: sp: 32 (over z, x), tp: 16 (over y, core).
Axes of the slice: x: 4, y: 8, z: 8, core: 2. Of those that a mesh axis runs over, the one named last changes fastest.
Arguments:
- tokens: bfloat16 [16384, 4096], P('sp', 'tp'), may hold values from -8 to 8
- w_key: bfloat16 [4096, 2048], P(None, 'tp'), may hold values from -0.09375 to 0.09375
- w_value: bfloat16 [4096, 2048], P(None, 'tp'), may hold values from -0.09375 to 0.09375
- w_beta: bfloat16 [4096, 16], replicated, may hold values from -0.09375 to 0.09375
- w_decay: bfloat16 [4096, 16], replicated, may hold values from -0.09375 to 0.09375
- beta_bias: float32 [16], replicated, may hold values from -6 to -4
- decay_rate: float32 [16], replicated, as said below
- forgetting_increment: float32 [16, 16384], P('tp', 'sp')
- new_query: bfloat16 [16, 128], P('tp', 'sp'), may hold values from -6 to 6
- read_gain: bfloat16 [128], replicated, may hold values from 0.099609375 to 1.8984375
Outputs:
- state_cache: bfloat16 [16, 128, 128], P('tp', 'sp')
- first_read: float32 [16, 128], P('tp')
The draws below stay inside these ranges and needn't reach their ends.
Inputs may be any that keep to these rules, and one draw needn't show every extreme that they name: `decay_rate`: positive.
All inputs are finite; a program needn't handle non-finite values.
Results may differ from the reference program's by a relative error of at most 0.0075.
Values may be sent and summed in bfloat16 or wider, within the bound.
A program may use at most 64 MiB of HBM per device.

```python
import math
import jax
import jax.numpy as jnp
from jax import lax

D = 4096
HEADS = 16
DK = 128
DV = 128
BLOCK = 64
LENGTH = 16384


def draw_tokens(key, part):
    perturbation_seed, common_key = jax.random.split(key, 2)
    blocks = LENGTH // BLOCK
    noise = jnp.clip(jax.random.normal(perturbation_seed, (LENGTH, D), jnp.float32), -4.5, 4.5)
    common = jnp.clip(jax.random.normal(common_key, (blocks, D), jnp.float32), -4.5, 4.5)
    mixed = noise + 0.7 * jnp.repeat(common, BLOCK, axis=0)
    return mixed.astype(jnp.bfloat16)


def draw_decay_rate(key, part):
    slow_key, fast_key, pick_key = jax.random.split(key, 3)
    slow = jnp.exp(jax.random.uniform(slow_key, (HEADS,), jnp.float32, math.log(0.2 / LENGTH), math.log(1.0 / LENGTH)))
    fast = jnp.exp(jax.random.uniform(fast_key, (HEADS,), jnp.float32, math.log(0.02), math.log(0.06)))
    picked = jax.random.bernoulli(pick_key, 0.5, (HEADS,))
    return jnp.where(picked, fast, slow)


def draw_forgetting_increment(key, part):
    scale_key, location_seed, drop_key = jax.random.split(key, 3)
    blocks = LENGTH // BLOCK
    factor = jnp.exp(jax.random.uniform(scale_key, (HEADS, blocks), jnp.float32, math.log(0.25), math.log(4.0)))
    starting_displacement = -jnp.repeat(factor, BLOCK, axis=1) / LENGTH
    location_positions = jax.random.randint(location_seed, (HEADS, 4), 0, LENGTH)
    discarded_elements = jnp.log(jax.random.uniform(drop_key, (HEADS, 4), jnp.float32, 0.5, 0.8))
    breadth_across = jnp.arange(LENGTH)
    cluster_batches = jnp.sum(jnp.where(breadth_across[None, None, :] == location_positions[:, :, None], discarded_elements[:, :, None], 0.0), axis=1)
    return starting_displacement + cluster_batches


def levels(stream_key, dims, shards, least, largest):
    level, own = 1.0, jax.random.fold_in(stream_key, 6)
    for dim, shards_of in shards:
        draws = jnp.exp(jax.random.uniform(jax.random.fold_in(own, dim), (shards_of,), jnp.float32, least / len(shards), largest / len(shards)))
        level = level * jnp.repeat(draws, dims[dim] // shards_of).reshape([-1 if axis == dim else 1 for axis in range(len(dims))])
    return level


def centred(own_key, shape, scale, limit, pieces=(), kind=jnp.bfloat16):
    array = jax.random.normal(own_key, shape, jnp.float32) * scale
    if len(pieces) > 0:
        array = levels(own_key, shape, pieces, -0.22, 0.18) * array
    return jnp.clip(array, min=-limit, max=limit).astype(kind)


def setup_inputs(seed: int = 0) -> dict:
    streams_of = jax.random.split(jax.random.key(seed), 11)
    return {
        "tokens": draw_tokens(jax.random.fold_in(streams_of[10], 71), 0),
        "w_key": centred(streams_of[1], (D, HEADS * DK), D ** -0.5, 0.09375, ((1, 16),)),
        "w_value": centred(streams_of[2], (D, HEADS * DV), D ** -0.5, 0.09375, ((1, 16),)),
        "w_beta": centred(streams_of[3], (D, HEADS), D ** -0.5, 0.09375),
        "w_decay": centred(streams_of[4], (D, HEADS), D ** -0.5, 0.09375),
        "beta_bias": jnp.clip(jax.random.uniform(streams_of[5], (HEADS,), jnp.float32, -6.0, -4.0), -6.0, -4.0),
        "decay_rate": draw_decay_rate(jax.random.fold_in(streams_of[10], 71), 0),
        "forgetting_increment": draw_forgetting_increment(jax.random.fold_in(streams_of[10], 71), 0),
        "new_query": centred(streams_of[8], (HEADS, DK), 1.0, 6.0, ((0, 16), (1, 32))),
        "read_gain": jnp.clip(1.0 + 0.18 * jax.random.normal(streams_of[9], (DV,), jnp.float32), 0.099609375, 1.8984375).astype(jnp.bfloat16),
    }


norm_eps = 1e-06

def matmul_f32(left, right):
    return jnp.dot(left, right, precision=lax.Precision.HIGHEST)

def unit_inverse(lower):
    current_size = lower.shape[0]
    identity = jnp.eye(current_size, dtype=jnp.float32)
    result = identity - lower
    lower_power = lower
    covered = 2
    while covered < current_size:
        lower_power = matmul_f32(lower_power, lower_power)
        result = matmul_f32(result, identity + lower_power)
        covered = covered * 2
    return result

def block_terms(key_blk, value_blk, beta_blk, logd_blk):
    current_size = key_blk.shape[0]
    cumulative = jnp.cumsum(logd_blk)
    spread = cumulative[:, None] - cumulative[None, :]
    location_positions = jnp.arange(current_size)
    causal = location_positions[:, None] >= location_positions[None, :]
    strict = location_positions[:, None] > location_positions[None, :]
    decay_table = jnp.where(causal, jnp.exp(jnp.where(causal, spread, 0.0)), 0.0)
    key_beta = key_blk * beta_blk[:, None]
    lower = jnp.where(strict, matmul_f32(key_beta, key_blk.T) * decay_table, 0.0)
    inverse = unit_inverse(lower)
    update = matmul_f32(inverse, value_blk * beta_blk[:, None])
    erase = matmul_f32(inverse, key_beta * jnp.exp(cumulative)[:, None])
    key_remainder = key_blk * jnp.exp(cumulative[-1] - cumulative)[:, None]
    return (update, erase, key_remainder, jnp.exp(cumulative[-1]))

def reference(tokens, w_key, w_value, w_beta, w_decay, beta_bias, decay_rate, forgetting_increment, new_query, read_gain):
    key_raw = jnp.dot(tokens, w_key, preferred_element_type=jnp.float32).astype(jnp.bfloat16)
    value_raw = jnp.dot(tokens, w_value, preferred_element_type=jnp.float32).astype(jnp.bfloat16)
    key_wide = lax.optimization_barrier(key_raw).astype(jnp.float32).reshape(LENGTH, HEADS, DK)
    key_unit = key_wide * lax.rsqrt(lax.optimization_barrier(jnp.sum(key_wide * key_wide, axis=-1, keepdims=True)) + norm_eps)
    value_wide = lax.optimization_barrier(value_raw).astype(jnp.float32).reshape(LENGTH, HEADS, DV)
    beta = jax.nn.sigmoid(jnp.dot(tokens, w_beta, preferred_element_type=jnp.float32) + beta_bias)
    log_decay = -decay_rate * jax.nn.softplus(jnp.dot(tokens, w_decay, preferred_element_type=jnp.float32)) + forgetting_increment.T
    blocks = LENGTH // BLOCK
    key_heads = key_unit.transpose(1, 0, 2).reshape(HEADS, blocks, BLOCK, DK)
    value_heads = value_wide.transpose(1, 0, 2).reshape(HEADS, blocks, BLOCK, DV)
    beta_heads = beta.T.reshape(HEADS, blocks, BLOCK)
    logd_heads = log_decay.T.reshape(HEADS, blocks, BLOCK)
    terms = jax.vmap(jax.vmap(block_terms))(key_heads, value_heads, beta_heads, logd_heads)
    inputs = tuple((jnp.moveaxis(item, 1, 0) for item in terms))

    def advance(state, block_in):
        update, erase, key_remainder, keep = block_in
        fresh = update - jnp.einsum('hcd,hde->hce', erase, state, precision=lax.Precision.HIGHEST)
        state = keep[:, None, None] * state + jnp.einsum('hcd,hce->hde', key_remainder, fresh, precision=lax.Precision.HIGHEST)
        return (state, None)
    final_state, _ = lax.scan(advance, jnp.zeros((HEADS, DK, DV), jnp.float32), inputs)
    state_cache = final_state.astype(jnp.bfloat16)
    raw_read = lax.optimization_barrier(jnp.sum(new_query.astype(jnp.float32)[:, :, None] * state_cache.astype(jnp.float32), axis=1))
    first_read = raw_read * lax.rsqrt(lax.optimization_barrier(jnp.mean(raw_read * raw_read, axis=-1, keepdims=True)) + norm_eps) * read_gain.astype(jnp.float32)
    return (state_cache, first_read)
```

```python
import functools

import jax
import jax.numpy as jnp
from jax import lax
from jax.experimental import pallas as pl
from jax.experimental.pallas import tpu as pltpu
from jax.sharding import PartitionSpec as P

NX, NZ, NY = 4, 8, 8
G = 4
R = 128
MESH = pl.DeviceIdType.MESH
f32, bf16 = jnp.float32, jnp.bfloat16
norm_eps = 1e-06


def nn(a, b):
    return lax.dot_general(a, b, (((1,), (0,)), ((), ())), preferred_element_type=f32)


def nt(a, b):
    return lax.dot_general(a, b, (((1,), (1,)), ((), ())), preferred_element_type=f32)


def tn(a, b):
    return lax.dot_general(a, b, (((0,), (0,)), ((), ())), preferred_element_type=f32)


def lo(x):
    return x.astype(bf16)


def iota(shape, dim):
    return lax.broadcasted_iota(jnp.int32, shape, dim)


def compose(first, second):
    nb1, a1, nb1_lo = first
    nb2, a2, nb2_lo = second
    q = nn(nb1_lo, nb2_lo[:R])
    n = a2 * nb1[:R] + a1 * nb2[:R] - q[:R]
    b = a2 * nb1[R:] - q[R:] + nb2[R:]
    return n, b, a1 * a2


def joined(n, b, a):
    nb = jnp.concatenate([n, b], axis=0)
    return nb, a, lo(nb)


def block_maps(kvs, gates, fincs, bias, rate):
    count = len(kvs)
    row, col = iota((R, R), 0), iota((R, R), 1)
    strict, causal = row > col, row >= col
    eye = (row == col).astype(f32)
    kw = [kv[:, :R].astype(bf16) for kv in kvs]
    vw = [kv[:, R:].astype(bf16) for kv in kvs]
    kk = [nt(k, k) for k in kw]
    rs = []
    for k in kw:
        wide = k.astype(f32)
        inv = lax.rsqrt(jnp.sum(wide * wide, axis=1, keepdims=True) + norm_eps)
        rs.append(jnp.broadcast_to(inv, (R, R)))
    rs_t = [r.T for r in rs]
    yield None
    beta, cum = [], []
    lane = iota((8, R), 1)
    for (bl, dl), finc in zip(gates, fincs):
        bl = jnp.broadcast_to(bl, (8, R))
        dl = jnp.broadcast_to(dl, (8, R))
        beta.append(jax.nn.sigmoid(bl + bias))
        c = -rate * jax.nn.softplus(dl) + jnp.broadcast_to(finc, (8, R))
        step = 1
        while step < R:
            c = c + jnp.where(lane >= step, pltpu.roll(c, step, 1), 0.0)
            step *= 2
        cum.append(c)
    beta_r = [jnp.broadcast_to(b[:1], (R, R)) for b in beta]
    cum_r = [jnp.broadcast_to(c[:1], (R, R)) for c in cum]
    beta_c = [b.T for b in beta_r]
    cum_c = [c.T for c in cum_r]
    yield None
    lower = []
    for i in range(count):
        spread = jnp.exp(jnp.where(causal, cum_c[i] - cum_r[i], 0.0))
        lower.append(jnp.where(strict, kk[i] * rs[i] * rs_t[i] * beta_c[i] * spread, 0.0))
    same = (row // 16) == (col // 16)
    power = [lo(jnp.where(same, l, 0.0)) for l in lower]
    inverse = [eye - jnp.where(same, l, 0.0) for l in lower]
    for _ in range(3):
        power = [lo(nn(p, p)) for p in power]
        inverse = [x + nn(lo(x), p) for x, p in zip(inverse, power)]
        yield None
    size = 16
    while size < R:
        below = ((row // (2 * size)) == (col // (2 * size))) & ((row // size) > (col // size))
        short = [lo(x) for x in inverse]
        inner = [lo(nn(s, lo(jnp.where(below, l, 0.0)))) for s, l in zip(short, lower)]
        inverse = [x - nn(y, s) for x, y, s in zip(inverse, inner, short)]
        size *= 2
        yield None
    maps = []
    for i in range(count):
        scale_u = beta_r[i]
        scale_e = scale_u * jnp.exp(cum_r[i]) * rs_t[i]
        erase = nn(lo(inverse[i] * scale_e), kw[i])
        update = nn(lo(inverse[i] * scale_u), vw[i])
        last = cum_c[i][R - 1 : R, :]
        remainder = lo(kw[i].astype(f32) * rs[i] * jnp.exp(last - cum_c[i]))
        n = tn(lo(erase), remainder)
        b = tn(lo(update), remainder)
        maps.append(joined(n, b, jnp.exp(last)))
    yield maps


def kernel(
    tok, wk, wv, wb, wd, bias_ref, rate_ref, finc, query, gain,
    state_out, read_out,
    x, wkv, wg, acc, accg, bfull, xs, ps, zs, fs, srow,
    load_sem, rsend, rrecv, dsend, drecv, xsend, xrecv, psem, zsend, zrecv, fsend, frecv,
):
    sp = lax.axis_index("sp")
    tp = lax.axis_index("tp")
    mz, mx = sp // NX, sp % NX
    my, core = tp // 2, tp % 2
    sigma = 2 * (mz % 2) - 1

    def at_y(step):
        return {"sp": sp, "tp": ((my + step + NY) % NY) * 2 + core}

    def at_x(step):
        return {"sp": mz * NX + (mx + step) % NX, "tp": tp}

    def at_z(step):
        return {"sp": ((mz + step + NZ) % NZ) * NX + mx, "tp": tp}

    other_core = {"sp": sp, "tp": my * 2 + 1 - core}
    pair = at_z(1 - 2 * (mz % 2))

    loads = []
    for g in range(G):
        c = pltpu.make_async_copy(
            tok.at[pl.ds(g * R, R)], x.at[tp, pl.ds(g * R, R)], load_sem.at[g]
        )
        c.start()
        loads.append(c)
    weights = [
        pltpu.make_async_copy(wk, wkv.at[:, pl.ds(0, R)], load_sem.at[G]),
        pltpu.make_async_copy(wv, wkv.at[:, pl.ds(R, R)], load_sem.at[G + 1]),
        pltpu.make_async_copy(wb, wg.at[pl.ds(0, 16)], load_sem.at[G + 2]),
        pltpu.make_async_copy(wd, wg.at[pl.ds(16, 16)], load_sem.at[G + 3]),
    ]
    for w in weights:
        w.start()

    barrier = pltpu.get_barrier_semaphore()
    peers = [at_y(1), at_y(-1), other_core, at_x(1), at_x(2), at_x(3)]
    z_peers = [at_z(sigma), at_z(3 * sigma), at_z(2 * sigma), at_z(-2 * sigma)]
    if True:
        z_peers.append(pair)
    for peer in peers + z_peers:
        pl.semaphore_signal(barrier, inc=1, device_id=peer, device_id_type=MESH)
    pl.semaphore_wait(barrier, len(peers) + len(z_peers))

    sent = []

    def shard(way, d, who):
        step = -d if way == 0 else d
        return ((my + step + NY) % NY) * 2 + who

    def rows(g):
        return pl.ds(g * R, R)

    def ring(way, d, g):
        s = shard(way, d, core)
        return pltpu.make_async_remote_copy(
            x.at[s, rows(g)], x.at[s, rows(g)],
            rsend.at[way, d, g], rrecv.at[way, d, g],
            device_id=at_y(1 if way == 0 else -1), device_id_type=MESH,
        )

    def send(way, d, g):
        c = ring(way, d, g)
        c.start()
        sent.append(c)

    def landed(way, d, g):
        s = shard(way, d, core)
        pltpu.make_async_remote_copy(
            x.at[s, rows(g)], x.at[s, rows(g)],
            rsend.at[way, d - 1, g], rrecv.at[way, d - 1, g],
            device_id=at_y(1 if way == 0 else -1), device_id_type=MESH,
        ).wait_recv()

    def across(way, d, g):
        s = shard(way, d, core)
        c = pltpu.make_async_remote_copy(
            x.at[s, rows(g)], x.at[s, rows(g)],
            dsend.at[way, d, g], drecv.at[way, d, g],
            device_id=other_core, device_id_type=MESH,
        )
        c.start()
        sent.append(c)

    def crossed(way, d, g):
        s = shard(way, d, 1 - core)
        pltpu.make_async_remote_copy(
            x.at[s, rows(g)], x.at[s, rows(g)],
            dsend.at[way, d, g], drecv.at[way, d, g],
            device_id=other_core, device_id_type=MESH,
        ).wait_recv()

    def project(items, g, first=False):
        total, gate = None, None
        for s in items:
            piece = x[s, g * R : (g + 1) * R, :]
            at = pl.multiple_of(s * 256, 256)
            p = nn(piece, wkv[pl.ds(at, 256), :])
            q = nt(wg[:, pl.ds(at, 256)], piece)
            total = p if total is None else total + p
            gate = q if gate is None else gate + q
        if first:
            acc[g * R : (g + 1) * R, :] = total
            accg[g] = gate
        else:
            acc[g * R : (g + 1) * R, :] += total
            accg[g] += gate

    pending = []

    def take_pending():
        while pending:
            items, g = pending.pop(0)
            for way, d in items:
                crossed(way, d, g)
            project([shard(way, d, 1 - core) for way, d in items], g)

    def event(items, g, forwards=True):
        for way, d in items:
            landed(way, d, g)
            if forwards and (d < 3 or (d == 3 and g % 2 == way)):
                send(way, d, g)
            across(way, d, g)

    def own_dots(items, g):
        project([shard(way, d, core) for way, d in items], g)
        take_pending()
        pending.append((items, g))

    both = lambda d: [(0, d), (1, d)]

    for g in (0, 1, 2, 3):
        loads[g].wait()
        if g < 3:
            send(0, 0, g)
            send(1, 0, g)
        across(0, 0, g)
    for w in weights:
        w.wait()
    for g in range(G):
        project([tp], g, first=True)

    h = tp
    bias, rate = bias_ref[h], rate_ref[h]

    def blocks_of(groups):
        kvs = [acc[g * R : (g + 1) * R, :] for g in groups]
        gates = [(accg[g, pl.ds(h, 1), :], accg[g, pl.ds(16 + h, 1), :]) for g in groups]
        fincs = [finc[:, g * R : (g + 1) * R] for g in groups]
        return block_maps(kvs, gates, fincs, bias, rate)

    pieces = None
    early = None

    def advance_early(n=1):
        nonlocal early
        for _ in range(n):
            if early is None:
                got = next(pieces)
                if got is not None:
                    early = joined(*compose(got[0], got[1]))

    event(both(1), 0)
    own_dots(both(1), 0)
    pending.append(([(0, 0)], 0))
    event(both(1), 1)
    send(0, 0, 3)
    send(1, 0, 3)
    own_dots(both(1), 1)
    pending.append(([(0, 0)], 1))
    event(both(2), 0)
    own_dots(both(2), 0)
    event(both(2), 1)
    own_dots(both(2), 1)
    event(both(1), 2)
    own_dots(both(1), 2)
    pending.append(([(0, 0)], 2))
    event(both(3), 0)
    event(both(3), 1)
    own_dots(both(3), 0)
    own_dots(both(3), 1)
    event(both(1), 3)
    own_dots(both(1), 3)
    pending.append(([(0, 0)], 3))
    event(both(2), 2)
    own_dots(both(2), 2)
    take_pending()
    event([(0, 4)], 0)
    event([(1, 4)], 1)
    own_dots([(0, 4)], 0)
    own_dots([(1, 4)], 1)
    take_pending()
    pieces = blocks_of((0, 1))
    advance_early(2)
    event(both(2), 3)
    own_dots(both(2), 3)
    advance_early(3)
    event(both(3), 2)
    own_dots(both(3), 2)
    advance_early(4)
    event(both(3), 3)
    own_dots(both(3), 3)
    take_pending()
    advance_early(4)
    event([(0, 4)], 2)
    event([(1, 4)], 3)
    own_dots([(0, 4)], 2)
    own_dots([(1, 4)], 3)
    take_pending()
    late = None
    for got in blocks_of((2, 3)):
        late = got
    n, b, a = compose(early, joined(*compose(late[0], late[1])))

    def keep_rows(keep, qrow):
        hi = keep.astype(bf16).astype(f32)
        mid = (keep - hi).astype(bf16).astype(f32)
        rest = keep - hi - mid
        r16 = iota((16, R), 0)
        blk = jnp.where(r16 == 0, hi, jnp.where(r16 == 1, mid, jnp.where(r16 == 2, rest, 0.0)))
        return lo(jnp.where(r16 == 3, qrow, blk))

    lane1 = iota((1, R), 1)
    q4 = query[...].astype(f32)
    qrow = jnp.zeros((1, R), f32)
    for i in range(4):
        qrow = qrow + jnp.where(lane1 == 4 * sp + i, q4[:, i : i + 1], 0.0)
    xs[mx, 0:R, :] = lo(n)
    xs[mx, R : R + 16, :] = keep_rows(a, qrow)
    bfull[...] = lo(b).reshape(NX, 32, R)
    sent_x = []
    for o in (2, 1, 3):
        c = pltpu.make_async_remote_copy(
            xs.at[mx, pl.ds(0, R + 16)], xs.at[mx, pl.ds(0, R + 16)],
            xsend.at[0, o - 1], xrecv.at[0, o - 1], device_id=at_x(o), device_id_type=MESH,
        )
        c.start()
        sent_x.append(c)
        c = pltpu.make_async_remote_copy(
            bfull.at[(mx + o) % NX], xs.at[mx, pl.ds(R + 16, 32)],
            xsend.at[1, o - 1], xrecv.at[1, o - 1], device_id=at_x(o), device_id_type=MESH,
        )
        c.start()
        sent_x.append(c)
    xs[mx, R + 16 : R + 48, :] = bfull[mx]

    def unpack(ref, k):
        n_lo = ref[k, 0:R, :]
        extra = ref[k, R : R + 16, :].astype(f32)
        b_lo = ref[k, R + 16 : R + 48, :]
        keep = extra[0:1] + extra[1:2] + extra[2:3]
        nb_lo = jnp.concatenate([n_lo, b_lo], axis=0)
        return (nb_lo.astype(f32), keep, nb_lo), extra[3:4]

    for o in (1, 3, 2):
        src = (mx + NX - o) % NX
        pltpu.make_async_remote_copy(
            xs.at[src, pl.ds(0, R + 16)], xs.at[src, pl.ds(0, R + 16)],
            xsend.at[0, o - 1], xrecv.at[0, o - 1], device_id=at_x(o), device_id_type=MESH,
        ).wait_recv()
        pltpu.make_async_remote_copy(
            bfull.at[0], xs.at[src, pl.ds(R + 16, 32)],
            xsend.at[1, o - 1], xrecv.at[1, o - 1], device_id=at_x(o), device_id_type=MESH,
        ).wait_recv()
    got = [unpack(xs, k) for k in range(NX)]
    half0 = joined(*compose(got[0][0], got[1][0]))
    half1 = joined(*compose(got[2][0], got[3][0]))
    n, b, a = compose(half0, half1)
    qrow = got[0][1] + got[1][1] + got[2][1] + got[3][1]

    def put(ref, slot, n, b, a, qrow):
        ref[slot, 0:R, :] = lo(n)
        ref[slot, R : R + 16, :] = keep_rows(a, qrow)
        ref[slot, R + 16 : R + 48, :] = lo(b)

    me2 = mz % 2
    put(ps, me2, n, b, a, qrow)
    c = pltpu.make_async_remote_copy(
        ps.at[me2], ps.at[me2], psem.at[0], psem.at[1], device_id=pair, device_id_type=MESH
    )
    c.start()
    sent_x.append(c)
    pltpu.make_async_remote_copy(
        ps.at[1 - me2], ps.at[1 - me2], psem.at[0], psem.at[1], device_id=pair, device_id_type=MESH
    ).wait_recv()
    got = [unpack(ps, k) for k in range(2)]
    n, b, a = compose(got[0][0], got[1][0])
    qrow = got[0][1] + got[1][1]

    mine = mz // 2
    put(zs, mine, n, b, a, qrow)
    for o in (3, 2, 1):
        c = pltpu.make_async_remote_copy(
            zs.at[mine], zs.at[mine], zsend.at[o - 1], zrecv.at[o - 1],
            device_id=at_z(o * sigma), device_id_type=MESH,
        )
        c.start()
        sent_x.append(c)
    for o, step in ((1, 1), (2, -2), (3, 3)):
        src = ((mz + step * sigma + NZ) % NZ) // 2
        pltpu.make_async_remote_copy(
            zs.at[src], zs.at[src], zsend.at[o - 1], zrecv.at[o - 1],
            device_id=at_z(o * sigma), device_id_type=MESH,
        ).wait_recv()
    got = [unpack(zs, k) for k in range(4)]
    state = got[0][0][0][R:]
    for k in range(1, 4):
        nb, keep, nb_lo = got[k][0]
        state = keep * state - nn(lo(state), nb_lo[:R]) + nb[R:]
    qrow = got[0][1] + got[1][1] + got[2][1] + got[3][1]

    fs[mx] = lo(state)
    for o in (2, 1, 3):
        c = pltpu.make_async_remote_copy(
            fs.at[mx], fs.at[mx], fsend.at[o - 1], frecv.at[o - 1],
            device_id=at_x(o), device_id_type=MESH,
        )
        c.start()
        sent_x.append(c)
    for o in (1, 3, 2):
        src = (mx + NX - o) % NX
        pltpu.make_async_remote_copy(
            fs.at[src], fs.at[src], fsend.at[o - 1], frecv.at[o - 1],
            device_id=at_x(o), device_id_type=MESH,
        ).wait_recv()
    whole = fs[...].reshape(R, R)
    raw = nt(jnp.broadcast_to(lo(qrow), (16, R)), whole)[0:1]
    gains = gain[...].astype(f32)
    read_out[...] = raw * lax.rsqrt(jnp.mean(raw * raw, axis=1, keepdims=True) + norm_eps) * gains
    srow[...] = whole.astype(f32).T
    state_out[0] = lo(srow[pl.ds(pl.multiple_of(4 * sp, 4), 4), :])

    for c in sent + sent_x:
        c.wait_send()


def per_device(tokens, w_key, w_value, w_beta, w_decay, beta_bias, decay_rate, finc, query, gain):
    hbm = pl.BlockSpec(memory_space=pl.ANY)
    vmem = pl.BlockSpec(memory_space=pltpu.VMEM)
    smem = pl.BlockSpec(memory_space=pltpu.SMEM)
    dma = pltpu.SemaphoreType.DMA
    return pl.pallas_call(
        kernel,
        out_shape=(
            jax.ShapeDtypeStruct((1, 4, R), bf16),
            jax.ShapeDtypeStruct((1, R), f32),
        ),
        in_specs=[hbm] * 5 + [smem, smem, vmem, vmem, vmem],
        out_specs=(vmem, vmem),
        scratch_shapes=[
            pltpu.VMEM((16, G * R, 256), bf16),
            pltpu.VMEM((4096, 256), bf16),
            pltpu.VMEM((32, 4096), bf16),
            pltpu.VMEM((G * R, 256), f32),
            pltpu.VMEM((G, 32, R), f32),
            pltpu.VMEM((NX, 32, R), bf16),
            pltpu.VMEM((NX, 176, R), bf16),
            pltpu.VMEM((2, 176, R), bf16),
            pltpu.VMEM((4, 176, R), bf16),
            pltpu.VMEM((NX, 32, R), bf16),
            pltpu.VMEM((R, R), f32),
            dma((G + 4,)),
            dma((2, 4, G)), dma((2, 4, G)),
            dma((2, 5, G)), dma((2, 5, G)),
            dma((2, 3)), dma((2, 3)),
            dma((2,)),
            dma((3,)), dma((3,)),
            dma((3,)), dma((3,)),
        ],
        compiler_params=pltpu.CompilerParams(
            collective_id=0, has_side_effects=True, vmem_limit_bytes=60 * 2**20
        ),
    )(
        tokens, w_key, w_value, w_beta.T, w_decay.T, beta_bias, decay_rate, finc, query,
        gain.reshape(1, R),
    )


def solution(mesh):
    return jax.shard_map(
        per_device,
        mesh=mesh,
        in_specs=(
            P("sp", "tp"),
            P(None, "tp"),
            P(None, "tp"),
            P(),
            P(),
            P(),
            P(),
            P("tp", "sp"),
            P("tp", "sp"),
            P(),
        ),
        out_specs=(P("tp", "sp", None), P("tp", None)),
        check_vma=False,
    )
```

```python
import functools

import jax
import jax.numpy as jnp
from jax import lax
from jax.experimental import pallas as pl
from jax.experimental.pallas import tpu as pltpu
from jax.sharding import PartitionSpec as P

NX, NZ, NY = 4, 8, 8
G = 4
R = 128
MESH = pl.DeviceIdType.MESH
f32, bf16 = jnp.float32, jnp.bfloat16
norm_eps = 1e-06


def nn(a, b):
    return lax.dot_general(a, b, (((1,), (0,)), ((), ())), preferred_element_type=f32)


def nt(a, b):
    return lax.dot_general(a, b, (((1,), (1,)), ((), ())), preferred_element_type=f32)


def tn(a, b):
    return lax.dot_general(a, b, (((0,), (0,)), ((), ())), preferred_element_type=f32)


def lo(x):
    return x.astype(bf16)


def iota(shape, dim):
    return lax.broadcasted_iota(jnp.int32, shape, dim)


def compose(first, second):
    nb1, a1, nb1_lo = first
    nb2, a2, nb2_lo = second
    q = nn(nb1_lo, nb2_lo[:R])
    n = a2 * nb1[:R] + a1 * nb2[:R] - q[:R]
    b = a2 * nb1[R:] - q[R:] + nb2[R:]
    return n, b, a1 * a2


def joined(n, b, a):
    nb = jnp.concatenate([n, b], axis=0)
    return nb, a, lo(nb)


def block_maps(kvs, gates, fincs, bias, rate):
    count = len(kvs)
    row, col = iota((R, R), 0), iota((R, R), 1)
    strict, causal = row > col, row >= col
    eye = (row == col).astype(f32)
    kw = [kv[:, :R].astype(bf16) for kv in kvs]
    vw = [kv[:, R:].astype(bf16) for kv in kvs]
    kk = [nt(k, k) for k in kw]
    rs = []
    for k in kw:
        wide = k.astype(f32)
        inv = lax.rsqrt(jnp.sum(wide * wide, axis=1, keepdims=True) + norm_eps)
        rs.append(jnp.broadcast_to(inv, (R, R)))
    rs_t = [r.T for r in rs]
    yield None
    beta, cum = [], []
    lane = iota((8, R), 1)
    for (bl, dl), finc in zip(gates, fincs):
        bl = jnp.broadcast_to(bl, (8, R))
        dl = jnp.broadcast_to(dl, (8, R))
        beta.append(jax.nn.sigmoid(bl + bias))
        c = -rate * jax.nn.softplus(dl) + jnp.broadcast_to(finc, (8, R))
        step = 1
        while step < R:
            c = c + jnp.where(lane >= step, pltpu.roll(c, step, 1), 0.0)
            step *= 2
        cum.append(c)
    beta_r = [jnp.broadcast_to(b[:1], (R, R)) for b in beta]
    cum_r = [jnp.broadcast_to(c[:1], (R, R)) for c in cum]
    beta_c = [b.T for b in beta_r]
    cum_c = [c.T for c in cum_r]
    yield None
    lower = []
    for i in range(count):
        spread = jnp.exp(jnp.where(causal, cum_c[i] - cum_r[i], 0.0))
        lower.append(jnp.where(strict, kk[i] * rs[i] * rs_t[i] * beta_c[i] * spread, 0.0))
    same = (row // 16) == (col // 16)
    power = [lo(jnp.where(same, l, 0.0)) for l in lower]
    inverse = [eye - jnp.where(same, l, 0.0) for l in lower]
    for _ in range(3):
        power = [lo(nn(p, p)) for p in power]
        inverse = [x + nn(lo(x), p) for x, p in zip(inverse, power)]
        yield None
    size = 16
    while size < R:
        below = ((row // (2 * size)) == (col // (2 * size))) & ((row // size) > (col // size))
        short = [lo(x) for x in inverse]
        inner = [lo(nn(s, lo(jnp.where(below, l, 0.0)))) for s, l in zip(short, lower)]
        inverse = [x - nn(y, s) for x, y, s in zip(inverse, inner, short)]
        size *= 2
        yield None
    maps = []
    for i in range(count):
        scale_u = beta_r[i]
        scale_e = scale_u * jnp.exp(cum_r[i]) * rs_t[i]
        erase = nn(lo(inverse[i] * scale_e), kw[i])
        update = nn(lo(inverse[i] * scale_u), vw[i])
        last = cum_c[i][R - 1 : R, :]
        remainder = lo(kw[i].astype(f32) * rs[i] * jnp.exp(last - cum_c[i]))
        n = tn(lo(erase), remainder)
        b = tn(lo(update), remainder)
        maps.append(joined(n, b, jnp.exp(last)))
    yield maps


def kernel(
    tok, wk, wv, wb, wd, bias_in, rate_in, finc_in, query_in, gain_in,
    packed,
    bias_ref, rate_ref, finc, query, gain,
    x, wkv, wg, acc, accg, bfull, xs, ps, zs, fs, srow,
    load_sem, rsend, rrecv, dsend, drecv, xsend, xrecv, psem, zsend, zrecv, fsend, frecv,
):
    sp = lax.axis_index("sp")
    tp = lax.axis_index("tp")
    mz, mx = sp // NX, sp % NX
    my, core = tp // 2, tp % 2
    sigma = 2 * (mz % 2) - 1

    def at_y(step):
        return {"sp": sp, "tp": ((my + step + NY) % NY) * 2 + core}

    def at_x(step):
        return {"sp": mz * NX + (mx + step) % NX, "tp": tp}

    def at_z(step):
        return {"sp": ((mz + step + NZ) % NZ) * NX + mx, "tp": tp}

    other_core = {"sp": sp, "tp": my * 2 + 1 - core}
    pair = at_z(1 - 2 * (mz % 2))

    loads = []
    for g in range(G):
        c = pltpu.make_async_copy(
            tok.at[pl.ds(g * R, R)], x.at[tp, pl.ds(g * R, R)], load_sem.at[g]
        )
        c.start()
        loads.append(c)
    weights = [
        pltpu.make_async_copy(wk, wkv.at[:, pl.ds(0, R)], load_sem.at[G]),
        pltpu.make_async_copy(wv, wkv.at[:, pl.ds(R, R)], load_sem.at[G + 1]),
        pltpu.make_async_copy(wb, wg.at[pl.ds(0, 16)], load_sem.at[G + 2]),
        pltpu.make_async_copy(wd, wg.at[pl.ds(16, 16)], load_sem.at[G + 3]),
    ]
    smalls = [
        pltpu.make_async_copy(src, dst, load_sem.at[G + 4 + i])
        for i, (src, dst) in enumerate((
            (bias_in, bias_ref), (rate_in, rate_ref), (finc_in, finc),
            (query_in, query), (gain_in, gain),
        ))
    ]
    for w in weights + smalls:
        w.start()

    barrier = pltpu.get_barrier_semaphore()
    peers = [at_y(1), at_y(-1), other_core, at_x(1), at_x(2), at_x(3)]
    z_peers = [at_z(sigma), at_z(3 * sigma), at_z(2 * sigma), at_z(-2 * sigma)]
    if True:
        z_peers.append(pair)
    for peer in peers + z_peers:
        pl.semaphore_signal(barrier, inc=1, device_id=peer, device_id_type=MESH)
    pl.semaphore_wait(barrier, len(peers) + len(z_peers))

    sent = []

    def shard(way, d, who):
        step = -d if way == 0 else d
        return ((my + step + NY) % NY) * 2 + who

    def rows(g):
        return pl.ds(g * R, R)

    def ring(way, d, g, sub):
        s = shard(way, d, core)
        part = x.at[s, pl.ds(g * R + sub * (R // 2), R // 2)]
        return pltpu.make_async_remote_copy(
            part, part, rsend.at[way, d, 2 * g + sub], rrecv.at[way, d, 2 * g + sub],
            device_id=at_y(1 if way == 0 else -1), device_id_type=MESH,
        )

    def landed(way, d, g, sub):
        s = shard(way, d, core)
        part = x.at[s, pl.ds(g * R + sub * (R // 2), R // 2)]
        pltpu.make_async_remote_copy(
            part, part, rsend.at[way, d - 1, 2 * g + sub], rrecv.at[way, d - 1, 2 * g + sub],
            device_id=at_y(1 if way == 0 else -1), device_id_type=MESH,
        ).wait_recv()

    def across(way, d, g):
        s = shard(way, d, core)
        c = pltpu.make_async_remote_copy(
            x.at[s, rows(g)], x.at[s, rows(g)],
            dsend.at[way, d, g], drecv.at[way, d, g],
            device_id=other_core, device_id_type=MESH,
        )
        c.start()
        sent.append(c)

    def crossed(way, d, g):
        s = shard(way, d, 1 - core)
        pltpu.make_async_remote_copy(
            x.at[s, rows(g)], x.at[s, rows(g)],
            dsend.at[way, d, g], drecv.at[way, d, g],
            device_id=other_core, device_id_type=MESH,
        ).wait_recv()

    def project(items, g, first=False):
        total, gate = None, None
        for s in items:
            piece = x[s, g * R : (g + 1) * R, :]
            at = pl.multiple_of(s * 256, 256)
            p = nn(piece, wkv[pl.ds(at, 256), :])
            q = nt(wg[:, pl.ds(at, 256)], piece)
            total = p if total is None else total + p
            gate = q if gate is None else gate + q
        if first:
            acc[g * R : (g + 1) * R, :] = total
            accg[g] = gate
        else:
            acc[g * R : (g + 1) * R, :] += total
            accg[g] += gate

    pending = []

    def take_pending(leave=0):
        while len(pending) > leave:
            way, d, g = pending.pop(0)
            crossed(way, d, g)
            project([shard(way, d, 1 - core)], g)

    def event(way, d, g, forward):
        for sub in range(2):
            landed(way, d, g, sub)
            if forward:
                c = ring(way, d, g, sub)
                c.start()
                sent.append(c)
        across(way, d, g)

    def step(d, half, leave=4):
        todo = []
        for way in range(2):
            g = half if way == 0 else half ^ 1
            event(way, d, g, d < 3 or (d == 3 and half % 2 == 0))
            todo.append((way, d, g))
        for way, d, g in todo:
            project([shard(way, d, core)], g)
            pending.append((way, d, g))
        take_pending(leave)

    def own(half):
        for way in range(2):
            g = half if way == 0 else half ^ 1
            for sub in range(2):
                c = ring(way, 0, g, sub)
                c.start()
                sent.append(c)

    loads[0].wait()
    loads[1].wait()
    own(0)
    own(1)
    across(0, 0, 0)
    across(0, 0, 1)
    loads[2].wait()
    loads[3].wait()
    across(0, 0, 2)
    across(0, 0, 3)
    for w in weights + smalls:
        w.wait()
    for g in range(G):
        project([tp], g, first=True)
        pending.append((0, 0, g))

    h = tp
    bias, rate = bias_ref[h], rate_ref[h]

    def blocks_of(groups):
        kvs = [acc[g * R : (g + 1) * R, :] for g in groups]
        gates = [(accg[g, pl.ds(h, 1), :], accg[g, pl.ds(16 + h, 1), :]) for g in groups]
        fincs = [finc[:, g * R : (g + 1) * R] for g in groups]
        return block_maps(kvs, gates, fincs, bias, rate)

    own(2)
    own(3)
    step(1, 0, 6)
    step(1, 1, 6)
    step(1, 2, 6)
    step(1, 3, 6)
    step(2, 0, 6)
    step(2, 1, 6)
    step(2, 2, 6)
    step(2, 3, 6)
    step(3, 0, 6)
    step(3, 1, 6)
    step(3, 2, 6)
    step(3, 3, 6)
    step(4, 0, 4)
    step(4, 2, 4)
    take_pending()
    late = None
    for got in blocks_of((0, 1, 2, 3)):
        late = got
    early = joined(*compose(late[0], late[1]))
    n, b, a = compose(early, joined(*compose(late[2], late[3])))

    def keep_rows(keep, qrow):
        hi = keep.astype(bf16).astype(f32)
        mid = (keep - hi).astype(bf16).astype(f32)
        rest = keep - hi - mid
        r16 = iota((16, R), 0)
        blk = jnp.where(r16 == 0, hi, jnp.where(r16 == 1, mid, jnp.where(r16 == 2, rest, 0.0)))
        return lo(jnp.where(r16 == 3, qrow, blk))

    lane1 = iota((1, R), 1)
    q4 = query[...].astype(f32)
    qrow = jnp.zeros((1, R), f32)
    for i in range(4):
        qrow = qrow + jnp.where(lane1 == 4 * sp + i, q4[:, i : i + 1], 0.0)
    xs[mx, 0:R, :] = lo(n)
    xs[mx, R : R + 16, :] = keep_rows(a, qrow)
    bfull[...] = lo(b).reshape(NX, 32, R)
    sent_x = []
    for o in (2, 1, 3):
        c = pltpu.make_async_remote_copy(
            xs.at[mx, pl.ds(0, R + 16)], xs.at[mx, pl.ds(0, R + 16)],
            xsend.at[0, o - 1], xrecv.at[0, o - 1], device_id=at_x(o), device_id_type=MESH,
        )
        c.start()
        sent_x.append(c)
        c = pltpu.make_async_remote_copy(
            bfull.at[(mx + o) % NX], xs.at[mx, pl.ds(R + 16, 32)],
            xsend.at[1, o - 1], xrecv.at[1, o - 1], device_id=at_x(o), device_id_type=MESH,
        )
        c.start()
        sent_x.append(c)
    xs[mx, R + 16 : R + 48, :] = bfull[mx]

    def unpack(ref, k):
        n_lo = ref[k, 0:R, :]
        extra = ref[k, R : R + 16, :].astype(f32)
        b_lo = ref[k, R + 16 : R + 48, :]
        keep = extra[0:1] + extra[1:2] + extra[2:3]
        nb_lo = jnp.concatenate([n_lo, b_lo], axis=0)
        return (nb_lo.astype(f32), keep, nb_lo), extra[3:4]

    for o in (1, 3, 2):
        src = (mx + NX - o) % NX
        pltpu.make_async_remote_copy(
            xs.at[src, pl.ds(0, R + 16)], xs.at[src, pl.ds(0, R + 16)],
            xsend.at[0, o - 1], xrecv.at[0, o - 1], device_id=at_x(o), device_id_type=MESH,
        ).wait_recv()
        pltpu.make_async_remote_copy(
            bfull.at[0], xs.at[src, pl.ds(R + 16, 32)],
            xsend.at[1, o - 1], xrecv.at[1, o - 1], device_id=at_x(o), device_id_type=MESH,
        ).wait_recv()
    got = [unpack(xs, k) for k in range(NX)]
    half0 = joined(*compose(got[0][0], got[1][0]))
    half1 = joined(*compose(got[2][0], got[3][0]))
    n, b, a = compose(half0, half1)
    qrow = got[0][1] + got[1][1] + got[2][1] + got[3][1]

    def put(ref, slot, n, b, a, qrow):
        ref[slot, 0:R, :] = lo(n)
        ref[slot, R : R + 16, :] = keep_rows(a, qrow)
        ref[slot, R + 16 : R + 48, :] = lo(b)

    me2 = mz % 2
    put(ps, me2, n, b, a, qrow)
    c = pltpu.make_async_remote_copy(
        ps.at[me2], ps.at[me2], psem.at[0], psem.at[1], device_id=pair, device_id_type=MESH
    )
    c.start()
    sent_x.append(c)
    pltpu.make_async_remote_copy(
        ps.at[1 - me2], ps.at[1 - me2], psem.at[0], psem.at[1], device_id=pair, device_id_type=MESH
    ).wait_recv()
    got = [unpack(ps, k) for k in range(2)]
    n, b, a = compose(got[0][0], got[1][0])
    qrow = got[0][1] + got[1][1]

    mine = mz // 2
    put(zs, mine, n, b, a, qrow)
    for o in (3, 2, 1):
        c = pltpu.make_async_remote_copy(
            zs.at[mine], zs.at[mine], zsend.at[o - 1], zrecv.at[o - 1],
            device_id=at_z(o * sigma), device_id_type=MESH,
        )
        c.start()
        sent_x.append(c)
    for o, step in ((1, 1), (2, -2), (3, 3)):
        src = ((mz + step * sigma + NZ) % NZ) // 2
        pltpu.make_async_remote_copy(
            zs.at[src], zs.at[src], zsend.at[o - 1], zrecv.at[o - 1],
            device_id=at_z(o * sigma), device_id_type=MESH,
        ).wait_recv()
    got = [unpack(zs, k) for k in range(4)]
    state = got[0][0][0][R:]
    for k in range(1, 4):
        nb, keep, nb_lo = got[k][0]
        state = keep * state - nn(lo(state), nb_lo[:R]) + nb[R:]
    qrow = got[0][1] + got[1][1] + got[2][1] + got[3][1]

    fs[mx] = lo(state)
    for o in (2, 1, 3):
        c = pltpu.make_async_remote_copy(
            fs.at[mx], fs.at[mx], fsend.at[o - 1], frecv.at[o - 1],
            device_id=at_x(o), device_id_type=MESH,
        )
        c.start()
        sent_x.append(c)
    for o in (1, 3, 2):
        src = (mx + NX - o) % NX
        pltpu.make_async_remote_copy(
            fs.at[src], fs.at[src], fsend.at[o - 1], frecv.at[o - 1],
            device_id=at_x(o), device_id_type=MESH,
        ).wait_recv()
    whole = fs[...].reshape(R, R)
    raw = nt(jnp.broadcast_to(lo(qrow), (16, R)), whole)[0:1]
    gains = gain[...].astype(f32)
    read = raw * lax.rsqrt(jnp.mean(raw * raw, axis=1, keepdims=True) + norm_eps) * gains
    srow[...] = whole.astype(f32).T
    packed[0:4, :] = srow[pl.ds(pl.multiple_of(4 * sp, 4), 4), :]
    packed[4:5, :] = read

    for c in sent + sent_x:
        c.wait_send()


def unpack_out(packed, state_out, read_out):
    state_out[0] = lo(packed[0:4, :])
    read_out[...] = packed[4:5, :]


def per_device(tokens, w_key, w_value, w_beta, w_decay, beta_bias, decay_rate, finc, query, gain):
    hbm = pl.BlockSpec(memory_space=pl.ANY)
    vmem = pl.BlockSpec(memory_space=pltpu.VMEM)
    dma = pltpu.SemaphoreType.DMA
    packed = pl.pallas_call(
        kernel,
        out_shape=jax.ShapeDtypeStruct((8, R), f32),
        in_specs=[hbm] * 10,
        out_specs=vmem,
        scratch_shapes=[
            pltpu.SMEM((16,), f32),
            pltpu.SMEM((16,), f32),
            pltpu.VMEM((1, G * R), f32),
            pltpu.VMEM((1, 4), bf16),
            pltpu.VMEM((1, R), bf16),
            pltpu.VMEM((16, G * R, 256), bf16),
            pltpu.VMEM((4096, 256), bf16),
            pltpu.VMEM((32, 4096), bf16),
            pltpu.VMEM((G * R, 256), f32),
            pltpu.VMEM((G, 32, R), f32),
            pltpu.VMEM((NX, 32, R), bf16),
            pltpu.VMEM((NX, 176, R), bf16),
            pltpu.VMEM((2, 176, R), bf16),
            pltpu.VMEM((4, 176, R), bf16),
            pltpu.VMEM((NX, 32, R), bf16),
            pltpu.VMEM((R, R), f32),
            dma((G + 9,)),
            dma((2, 4, 2 * G)), dma((2, 4, 2 * G)),
            dma((2, 5, G)), dma((2, 5, G)),
            dma((2, 3)), dma((2, 3)),
            dma((2,)),
            dma((3,)), dma((3,)),
            dma((3,)), dma((3,)),
        ],
        compiler_params=pltpu.CompilerParams(
            collective_id=0, has_side_effects=True, vmem_limit_bytes=60 * 2**20
        ),
    )(
        tokens, w_key, w_value, w_beta.T, w_decay.T, beta_bias, decay_rate, finc, query,
        gain.reshape(1, R),
    )
    return pl.pallas_call(
        unpack_out,
        out_shape=(
            jax.ShapeDtypeStruct((1, 4, R), bf16),
            jax.ShapeDtypeStruct((1, R), f32),
        ),
        in_specs=[vmem],
        out_specs=(vmem, vmem),
    )(packed)


def solution(mesh):
    return jax.shard_map(
        per_device,
        mesh=mesh,
        in_specs=(
            P("sp", "tp"),
            P(None, "tp"),
            P(None, "tp"),
            P(),
            P(),
            P(),
            P(),
            P("tp", "sp"),
            P("tp", "sp"),
            P(),
        ),
        out_specs=(P("tp", "sp", None), P("tp", None)),
        check_vma=False,
    )
```

```python
import functools

import jax
import jax.numpy as jnp
from jax import lax
from jax.experimental import pallas as pl
from jax.experimental.pallas import tpu as pltpu
from jax.sharding import PartitionSpec as P

NX, NZ, NY = 4, 8, 8
G = 4
R = 128
MESH = pl.DeviceIdType.MESH
f32, bf16 = jnp.float32, jnp.bfloat16
norm_eps = 1e-06


def nn(a, b):
    return lax.dot_general(a, b, (((1,), (0,)), ((), ())), preferred_element_type=f32)


def nt(a, b):
    return lax.dot_general(a, b, (((1,), (1,)), ((), ())), preferred_element_type=f32)


def tn(a, b):
    return lax.dot_general(a, b, (((0,), (0,)), ((), ())), preferred_element_type=f32)


def lo(x):
    return x.astype(bf16)


def iota(shape, dim):
    return lax.broadcasted_iota(jnp.int32, shape, dim)


def compose(first, second):
    nb1, a1, nb1_lo = first
    nb2, a2, nb2_lo = second
    q = nn(nb1_lo, nb2_lo[:R])
    n = a2 * nb1[:R] + a1 * nb2[:R] - q[:R]
    b = a2 * nb1[R:] - q[R:] + nb2[R:]
    return n, b, a1 * a2


def joined(n, b, a):
    nb = jnp.concatenate([n, b], axis=0)
    return nb, a, lo(nb)


def block_maps(kvs, gates, fincs, bias, rate):
    count = len(kvs)
    row, col = iota((R, R), 0), iota((R, R), 1)
    strict = row > col
    eye = (row == col).astype(f32)
    kw = [kv[:, :R].astype(bf16) for kv in kvs]
    kk = [nt(k, k) for k in kw]
    logits = jnp.concatenate([dl for _, dl in gates] + [bl for bl, _ in gates], axis=0)
    c = -rate * jax.nn.softplus(logits) + jnp.concatenate(fincs + fincs, axis=0)
    beta = jax.nn.sigmoid(logits + bias)
    lane = iota((2 * count, R), 1)
    step = 1
    while step < R:
        c = c + jnp.where(lane >= step, pltpu.roll(c, step, 1), 0.0)
        step *= 2
    packed = jnp.where(iota((2 * count, R), 0) < count, c, beta)
    columns = packed.T
    rs, spread_rs = [], jnp.zeros((R, R), f32)
    for i, k in enumerate(kw):
        wide = k.astype(f32)
        rs.append(lax.rsqrt(jnp.sum(wide * wide, axis=1, keepdims=True) + norm_eps))
        spread_rs = jnp.where(col == i, rs[i], spread_rs)
    rs_rows = spread_rs.T
    cum_r = [packed[i : i + 1] for i in range(count)]
    cum_c = [columns[:, i : i + 1] for i in range(count)]
    beta_r = [packed[count + i : count + i + 1] for i in range(count)]
    beta_c = [columns[:, count + i : count + i + 1] for i in range(count)]
    rs_r = [rs_rows[i : i + 1] for i in range(count)]
    lower = []
    for i in range(count):
        decay = jnp.exp(jnp.where(strict, cum_c[i] - cum_r[i], 0.0))
        lower.append(jnp.where(strict, kk[i] * (rs[i] * beta_c[i]) * rs_r[i] * decay, 0.0))
    same = (row // 16) == (col // 16)
    power = [lo(jnp.where(same, l, 0.0)) for l in lower]
    inverse = [eye - jnp.where(same, l, 0.0) for l in lower]
    for _ in range(3):
        power = [lo(nn(p, p)) for p in power]
        inverse = [x + nn(lo(x), p) for x, p in zip(inverse, power)]
    size = 16
    while size < R:
        below = ((row // (2 * size)) == (col // (2 * size))) & ((row // size) > (col // size))
        short = [lo(x) for x in inverse]
        inner = [lo(nn(s, lo(jnp.where(below, l, 0.0)))) for s, l in zip(short, lower)]
        inverse = [x - nn(y, s) for x, y, s in zip(inverse, inner, short)]
        size *= 2
    ns, keeps, remainders = [], [], []
    for i in range(count):
        last = cum_r[i][:, R - 1 : R]
        keeps.append(jnp.broadcast_to(jnp.exp(last), (1, R)))
        remainders.append(lo(kw[i].astype(f32) * (rs[i] * jnp.exp(last - cum_c[i]))))
        erase = nn(lo(inverse[i] * (beta_r[i] * jnp.exp(cum_r[i]) * rs_r[i])), kw[i])
        ns.append(tn(lo(erase), remainders[i]))

    def values():
        bs = []
        for i in range(count):
            update = nn(lo(inverse[i] * beta_r[i]), kvs[i][:, R:].astype(bf16))
            bs.append(tn(lo(update), remainders[i]))
        return bs

    return ns, keeps, values


def kernel(
    tok, wk, wv, wb, wd, bias_in, rate_in, finc_in, query_in, gain_in,
    packed,
    bias_ref, rate_ref, finc, query, gain,
    x, wkv, wg, acc, accg, bfull, xs, ps, zs, fs, srow,
    load_sem, rsend, rrecv, dsend, drecv, xsend, xrecv, psem, zsend, zrecv, fsend, frecv,
):
    sp = lax.axis_index("sp")
    tp = lax.axis_index("tp")
    mz, mx = sp // NX, sp % NX
    my, core = tp // 2, tp % 2
    sigma = 2 * (mz % 2) - 1

    def at_y(step):
        return {"sp": sp, "tp": ((my + step + NY) % NY) * 2 + core}

    def at_x(step):
        return {"sp": mz * NX + (mx + step) % NX, "tp": tp}

    def at_z(step):
        return {"sp": ((mz + step + NZ) % NZ) * NX + mx, "tp": tp}

    other_core = {"sp": sp, "tp": my * 2 + 1 - core}
    pair = at_z(1 - 2 * (mz % 2))

    loads = []
    for g in range(G):
        c = pltpu.make_async_copy(
            tok.at[pl.ds(g * R, R)], x.at[tp, pl.ds(g * R, R)], load_sem.at[g]
        )
        c.start()
        loads.append(c)
    weights = [
        pltpu.make_async_copy(wk, wkv.at[:, pl.ds(0, R)], load_sem.at[G]),
        pltpu.make_async_copy(wv, wkv.at[:, pl.ds(R, R)], load_sem.at[G + 1]),
        pltpu.make_async_copy(wb, wg.at[pl.ds(0, 16)], load_sem.at[G + 2]),
        pltpu.make_async_copy(wd, wg.at[pl.ds(16, 16)], load_sem.at[G + 3]),
    ]
    smalls = [
        pltpu.make_async_copy(src, dst, load_sem.at[G + 4 + i])
        for i, (src, dst) in enumerate((
            (bias_in, bias_ref), (rate_in, rate_ref), (finc_in, finc),
            (query_in, query), (gain_in, gain),
        ))
    ]

    barrier = pltpu.get_barrier_semaphore()
    peers = [at_y(1), at_y(-1), other_core, at_x(1), at_x(2), at_x(3)]
    z_peers = [at_z(sigma), at_z(3 * sigma), at_z(2 * sigma), at_z(-2 * sigma)]
    if True:
        z_peers.append(pair)
    for peer in peers + z_peers:
        pl.semaphore_signal(barrier, inc=1, device_id=peer, device_id_type=MESH)
    pl.semaphore_wait(barrier, len(peers) + len(z_peers))

    sent = []

    def shard(way, d, who):
        step = -d if way == 0 else d
        return ((my + step + NY) % NY) * 2 + who

    def rows(g):
        return pl.ds(g * R, R)

    def ring(way, d, g, sub):
        s = shard(way, d, core)
        part = x.at[s, pl.ds(g * R + sub * (R // 2), R // 2)]
        return pltpu.make_async_remote_copy(
            part, part, rsend.at[way, d, 2 * g + sub], rrecv.at[way, d, 2 * g + sub],
            device_id=at_y(1 if way == 0 else -1), device_id_type=MESH,
        )

    def landed(way, d, g, sub):
        s = shard(way, d, core)
        part = x.at[s, pl.ds(g * R + sub * (R // 2), R // 2)]
        pltpu.make_async_remote_copy(
            part, part, rsend.at[way, d - 1, 2 * g + sub], rrecv.at[way, d - 1, 2 * g + sub],
            device_id=at_y(1 if way == 0 else -1), device_id_type=MESH,
        ).wait_recv()

    def across(way, d, g):
        s = shard(way, d, core)
        c = pltpu.make_async_remote_copy(
            x.at[s, rows(g)], x.at[s, rows(g)],
            dsend.at[way, d, g], drecv.at[way, d, g],
            device_id=other_core, device_id_type=MESH,
        )
        c.start()
        sent.append(c)

    def crossed(way, d, g):
        s = shard(way, d, 1 - core)
        pltpu.make_async_remote_copy(
            x.at[s, rows(g)], x.at[s, rows(g)],
            dsend.at[way, d, g], drecv.at[way, d, g],
            device_id=other_core, device_id_type=MESH,
        ).wait_recv()

    def project(items, g, first=False):
        total, gate = None, None
        for s in items:
            piece = x[s, g * R : (g + 1) * R, :]
            at = pl.multiple_of(s * 256, 256)
            p = nn(piece, wkv[pl.ds(at, 256), :])
            q = nt(wg[:, pl.ds(at, 256)], piece)
            total = p if total is None else total + p
            gate = q if gate is None else gate + q
        if first:
            acc[g * R : (g + 1) * R, :] = total
            accg[g] = gate
        else:
            acc[g * R : (g + 1) * R, :] += total
            accg[g] += gate

    pending = []

    def take_pending(leave=0):
        while len(pending) > leave:
            way, d, g = pending.pop(0)
            crossed(way, d, g)
            project([shard(way, d, 1 - core)], g)

    def event(way, d, g, forward):
        for sub in range(2):
            landed(way, d, g, sub)
            if forward:
                c = ring(way, d, g, sub)
                c.start()
                sent.append(c)
        across(way, d, g)

    def step(d, half, leave=4):
        todo = []
        for way in range(2):
            g = half if way == 0 else half ^ 1
            event(way, d, g, d < 3 or (d == 3 and half % 2 == 0))
            todo.append((way, d, g))
        for way, d, g in todo:
            project([shard(way, d, core)], g)
            pending.append((way, d, g))
        take_pending(leave)

    def own(half):
        for way in range(2):
            g = half if way == 0 else half ^ 1
            for sub in range(2):
                c = ring(way, 0, g, sub)
                c.start()
                sent.append(c)

    loads[0].wait()
    loads[1].wait()
    own(0)
    own(1)
    across(0, 0, 0)
    across(0, 0, 1)
    for w in weights + smalls:
        w.start()
    loads[2].wait()
    loads[3].wait()
    across(0, 0, 2)
    across(0, 0, 3)
    for w in weights + smalls:
        w.wait()
    for g in range(G):
        project([tp], g, first=True)
        pending.append((0, 0, g))

    h = tp
    bias, rate = bias_ref[h], rate_ref[h]

    def blocks_of(groups):
        kvs = [acc[g * R : (g + 1) * R, :] for g in groups]
        gates = [(accg[g, pl.ds(h, 1), :], accg[g, pl.ds(16 + h, 1), :]) for g in groups]
        fincs = [finc[:, g * R : (g + 1) * R] for g in groups]
        return block_maps(kvs, gates, fincs, bias, rate)

    own(2)
    own(3)
    step(1, 0, 6)
    step(1, 1, 6)
    step(1, 2, 6)
    step(1, 3, 6)
    step(2, 0, 6)
    step(2, 1, 6)
    step(2, 2, 6)
    step(2, 3, 6)
    step(3, 0, 6)
    step(3, 1, 6)
    step(3, 2, 6)
    step(3, 3, 6)
    step(4, 0, 4)
    step(4, 2, 4)
    take_pending()
    late = None
    ns, keeps, values = blocks_of((0, 1, 2, 3))

    def n_of(n1, a1, n2, a2):
        return a2 * n1 + a1 * n2 - nn(lo(n1), lo(n2))

    n01, a01 = n_of(ns[0], keeps[0], ns[1], keeps[1]), keeps[0] * keeps[1]
    n23, a23 = n_of(ns[2], keeps[2], ns[3], keeps[3]), keeps[2] * keeps[3]
    n, a = n_of(n01, a01, n23, a23), a01 * a23

    def keep_rows(keep, qrow):
        hi = keep.astype(bf16).astype(f32)
        mid = (keep - hi).astype(bf16).astype(f32)
        rest = keep - hi - mid
        r16 = iota((16, R), 0)
        blk = jnp.where(r16 == 0, hi, jnp.where(r16 == 1, mid, jnp.where(r16 == 2, rest, 0.0)))
        return lo(jnp.where(r16 == 3, qrow, blk))

    lane1 = iota((1, R), 1)
    q4 = query[...].astype(f32)
    qrow = jnp.zeros((1, R), f32)
    for i in range(4):
        qrow = qrow + jnp.where(lane1 == 4 * sp + i, q4[:, i : i + 1], 0.0)
    xs[mx, 0:R, :] = lo(n)
    xs[mx, R : R + 16, :] = keep_rows(a, qrow)
    sent_x = []
    for o in (2, 1, 3):
        c = pltpu.make_async_remote_copy(
            xs.at[mx, pl.ds(0, R + 16)], xs.at[mx, pl.ds(0, R + 16)],
            xsend.at[0, o - 1], xrecv.at[0, o - 1], device_id=at_x(o), device_id_type=MESH,
        )
        c.start()
        sent_x.append(c)
    bs = values()

    def b_of(b1, n2, a2, b2):
        return a2 * b1 - nn(lo(b1), lo(n2)) + b2

    b01 = b_of(bs[0], ns[1], keeps[1], bs[1])
    b23 = b_of(bs[2], ns[3], keeps[3], bs[3])
    b = b_of(b01, n23, a23, b23)
    bfull[...] = lo(b).reshape(NX, 32, R)
    for o in (2, 1, 3):
        c = pltpu.make_async_remote_copy(
            bfull.at[(mx + o) % NX], xs.at[mx, pl.ds(R + 16, 32)],
            xsend.at[1, o - 1], xrecv.at[1, o - 1], device_id=at_x(o), device_id_type=MESH,
        )
        c.start()
        sent_x.append(c)
    xs[mx, R + 16 : R + 48, :] = bfull[mx]

    def unpack(ref, k):
        n_lo = ref[k, 0:R, :]
        extra = ref[k, R : R + 16, :].astype(f32)
        b_lo = ref[k, R + 16 : R + 48, :]
        keep = extra[0:1] + extra[1:2] + extra[2:3]
        nb_lo = jnp.concatenate([n_lo, b_lo], axis=0)
        return (nb_lo.astype(f32), keep, nb_lo), extra[3:4]

    for o in (1, 3, 2):
        src = (mx + NX - o) % NX
        pltpu.make_async_remote_copy(
            xs.at[src, pl.ds(0, R + 16)], xs.at[src, pl.ds(0, R + 16)],
            xsend.at[0, o - 1], xrecv.at[0, o - 1], device_id=at_x(o), device_id_type=MESH,
        ).wait_recv()
        pltpu.make_async_remote_copy(
            bfull.at[0], xs.at[src, pl.ds(R + 16, 32)],
            xsend.at[1, o - 1], xrecv.at[1, o - 1], device_id=at_x(o), device_id_type=MESH,
        ).wait_recv()
    got = [unpack(xs, k) for k in range(NX)]
    half0 = joined(*compose(got[0][0], got[1][0]))
    half1 = joined(*compose(got[2][0], got[3][0]))
    n, b, a = compose(half0, half1)
    qrow = got[0][1] + got[1][1] + got[2][1] + got[3][1]

    def put(ref, slot, n, b, a, qrow):
        ref[slot, 0:R, :] = lo(n)
        ref[slot, R : R + 16, :] = keep_rows(a, qrow)
        ref[slot, R + 16 : R + 48, :] = lo(b)

    me2 = mz % 2
    put(ps, me2, n, b, a, qrow)
    c = pltpu.make_async_remote_copy(
        ps.at[me2], ps.at[me2], psem.at[0], psem.at[1], device_id=pair, device_id_type=MESH
    )
    c.start()
    sent_x.append(c)
    pltpu.make_async_remote_copy(
        ps.at[1 - me2], ps.at[1 - me2], psem.at[0], psem.at[1], device_id=pair, device_id_type=MESH
    ).wait_recv()
    got = [unpack(ps, k) for k in range(2)]
    n, b, a = compose(got[0][0], got[1][0])
    qrow = got[0][1] + got[1][1]

    mine = mz // 2
    put(zs, mine, n, b, a, qrow)
    for o in (3, 2, 1):
        c = pltpu.make_async_remote_copy(
            zs.at[mine], zs.at[mine], zsend.at[o - 1], zrecv.at[o - 1],
            device_id=at_z(o * sigma), device_id_type=MESH,
        )
        c.start()
        sent_x.append(c)
    for o, step in ((1, 1), (2, -2), (3, 3)):
        src = ((mz + step * sigma + NZ) % NZ) // 2
        pltpu.make_async_remote_copy(
            zs.at[src], zs.at[src], zsend.at[o - 1], zrecv.at[o - 1],
            device_id=at_z(o * sigma), device_id_type=MESH,
        ).wait_recv()
    got = [unpack(zs, k) for k in range(4)]
    state = got[0][0][0][R:]
    for k in range(1, 4):
        nb, keep, nb_lo = got[k][0]
        state = keep * state - nn(lo(state), nb_lo[:R]) + nb[R:]
    qrow = got[0][1] + got[1][1] + got[2][1] + got[3][1]

    fs[mx] = lo(state)
    for o in (2, 1, 3):
        c = pltpu.make_async_remote_copy(
            fs.at[mx], fs.at[mx], fsend.at[o - 1], frecv.at[o - 1],
            device_id=at_x(o), device_id_type=MESH,
        )
        c.start()
        sent_x.append(c)
    for o in (1, 3, 2):
        src = (mx + NX - o) % NX
        pltpu.make_async_remote_copy(
            fs.at[src], fs.at[src], fsend.at[o - 1], frecv.at[o - 1],
            device_id=at_x(o), device_id_type=MESH,
        ).wait_recv()
    whole = fs[...].reshape(R, R)
    raw = nt(jnp.broadcast_to(lo(qrow), (16, R)), whole)[0:1]
    gains = gain[...].astype(f32)
    read = raw * lax.rsqrt(jnp.mean(raw * raw, axis=1, keepdims=True) + norm_eps) * gains
    srow[...] = whole.astype(f32).T
    packed[0:4, :] = srow[pl.ds(pl.multiple_of(4 * sp, 4), 4), :]
    packed[4:5, :] = read

    for c in sent + sent_x:
        c.wait_send()


def unpack_out(packed, state_out, read_out):
    state_out[0] = lo(packed[0:4, :])
    read_out[...] = packed[4:5, :]


def per_device(tokens, w_key, w_value, w_beta, w_decay, beta_bias, decay_rate, finc, query, gain):
    hbm = pl.BlockSpec(memory_space=pl.ANY)
    vmem = pl.BlockSpec(memory_space=pltpu.VMEM)
    dma = pltpu.SemaphoreType.DMA
    packed = pl.pallas_call(
        kernel,
        out_shape=jax.ShapeDtypeStruct((8, R), f32),
        in_specs=[hbm] * 10,
        out_specs=vmem,
        scratch_shapes=[
            pltpu.SMEM((16,), f32),
            pltpu.SMEM((16,), f32),
            pltpu.VMEM((1, G * R), f32),
            pltpu.VMEM((1, 4), bf16),
            pltpu.VMEM((1, R), bf16),
            pltpu.VMEM((16, G * R, 256), bf16),
            pltpu.VMEM((4096, 256), bf16),
            pltpu.VMEM((32, 4096), bf16),
            pltpu.VMEM((G * R, 256), f32),
            pltpu.VMEM((G, 32, R), f32),
            pltpu.VMEM((NX, 32, R), bf16),
            pltpu.VMEM((NX, 176, R), bf16),
            pltpu.VMEM((2, 176, R), bf16),
            pltpu.VMEM((4, 176, R), bf16),
            pltpu.VMEM((NX, 32, R), bf16),
            pltpu.VMEM((R, R), f32),
            dma((G + 9,)),
            dma((2, 4, 2 * G)), dma((2, 4, 2 * G)),
            dma((2, 5, G)), dma((2, 5, G)),
            dma((2, 3)), dma((2, 3)),
            dma((2,)),
            dma((3,)), dma((3,)),
            dma((3,)), dma((3,)),
        ],
        compiler_params=pltpu.CompilerParams(
            collective_id=0, has_side_effects=True, vmem_limit_bytes=60 * 2**20
        ),
    )(
        tokens, w_key, w_value, w_beta.T, w_decay.T, beta_bias, decay_rate, finc, query,
        gain.reshape(1, R),
    )
    return pl.pallas_call(
        unpack_out,
        out_shape=(
            jax.ShapeDtypeStruct((1, 4, R), bf16),
            jax.ShapeDtypeStruct((1, R), f32),
        ),
        in_specs=[vmem],
        out_specs=(vmem, vmem),
    )(packed)


def solution(mesh):
    return jax.shard_map(
        per_device,
        mesh=mesh,
        in_specs=(
            P("sp", "tp"),
            P(None, "tp"),
            P(None, "tp"),
            P(),
            P(),
            P(),
            P(),
            P("tp", "sp"),
            P("tp", "sp"),
            P(),
        ),
        out_specs=(P("tp", "sp", None), P("tp", None)),
        check_vma=False,
    )
```

```python
import functools

import jax
import jax.numpy as jnp
from jax import lax
from jax.experimental import pallas as pl
from jax.experimental.pallas import tpu as pltpu
from jax.sharding import PartitionSpec as P

NX, NZ, NY = 4, 8, 8
G = 4
R = 128
MESH = pl.DeviceIdType.MESH
f32, bf16 = jnp.float32, jnp.bfloat16
norm_eps = 1e-06


def nn(a, b):
    return lax.dot_general(a, b, (((1,), (0,)), ((), ())), preferred_element_type=f32)


def nt(a, b):
    return lax.dot_general(a, b, (((1,), (1,)), ((), ())), preferred_element_type=f32)


def tn(a, b):
    return lax.dot_general(a, b, (((0,), (0,)), ((), ())), preferred_element_type=f32)


def lo(x):
    return x.astype(bf16)


def iota(shape, dim):
    return lax.broadcasted_iota(jnp.int32, shape, dim)


def compose(first, second):
    nb1, a1, nb1_lo = first
    nb2, a2, nb2_lo = second
    q = nn(nb1_lo, nb2_lo[:R])
    n = a2 * nb1[:R] + a1 * nb2[:R] - q[:R]
    b = a2 * nb1[R:] - q[R:] + nb2[R:]
    return n, b, a1 * a2


def joined(n, b, a):
    nb = jnp.concatenate([n, b], axis=0)
    return nb, a, lo(nb)


def block_maps(kvs, gates, fincs, bias, rate):
    count = len(kvs)
    row, col = iota((R, R), 0), iota((R, R), 1)
    strict = row > col
    eye = (row == col).astype(f32)
    kw = [kv[:, :R].astype(bf16) for kv in kvs]
    kk = [nt(k, k) for k in kw]
    logits = jnp.concatenate([dl for _, dl in gates] + [bl for bl, _ in gates], axis=0)
    c = -rate * jax.nn.softplus(logits) + jnp.concatenate(fincs + fincs, axis=0)
    beta = jax.nn.sigmoid(logits + bias)
    lane = iota((2 * count, R), 1)
    step = 1
    while step < R:
        c = c + jnp.where(lane >= step, pltpu.roll(c, step, 1), 0.0)
        step *= 2
    packed = jnp.where(iota((2 * count, R), 0) < count, c, beta)
    columns = packed.T
    rs, spread_rs = [], jnp.zeros((R, R), f32)
    for i, k in enumerate(kw):
        wide = k.astype(f32)
        rs.append(lax.rsqrt(jnp.sum(wide * wide, axis=1, keepdims=True) + norm_eps))
        spread_rs = jnp.where(col == i, rs[i], spread_rs)
    rs_rows = spread_rs.T
    cum_r = [packed[i : i + 1] for i in range(count)]
    cum_c = [columns[:, i : i + 1] for i in range(count)]
    beta_r = [packed[count + i : count + i + 1] for i in range(count)]
    beta_c = [columns[:, count + i : count + i + 1] for i in range(count)]
    rs_r = [rs_rows[i : i + 1] for i in range(count)]
    lower = []
    for i in range(count):
        decay = jnp.exp(jnp.where(strict, cum_c[i] - cum_r[i], 0.0))
        lower.append(jnp.where(strict, kk[i] * (rs[i] * beta_c[i]) * rs_r[i] * decay, 0.0))
    same = (row // 16) == (col // 16)
    power = [lo(jnp.where(same, l, 0.0)) for l in lower]
    inverse = [eye - jnp.where(same, l, 0.0) for l in lower]
    for _ in range(3):
        power = [lo(nn(p, p)) for p in power]
        inverse = [x + nn(lo(x), p) for x, p in zip(inverse, power)]
    size = 16
    while size < R:
        below = ((row // (2 * size)) == (col // (2 * size))) & ((row // size) > (col // size))
        short = [lo(x) for x in inverse]
        inner = [lo(nn(s, lo(jnp.where(below, l, 0.0)))) for s, l in zip(short, lower)]
        inverse = [x - nn(y, s) for x, y, s in zip(inverse, inner, short)]
        size *= 2
    ns, keeps, remainders = [], [], []
    for i in range(count):
        last = cum_r[i][:, R - 1 : R]
        keeps.append(jnp.broadcast_to(jnp.exp(last), (1, R)))
        remainders.append(lo(kw[i].astype(f32) * (rs[i] * jnp.exp(last - cum_c[i]))))
        erase = nn(lo(inverse[i] * (beta_r[i] * jnp.exp(cum_r[i]) * rs_r[i])), kw[i])
        ns.append(tn(lo(erase), remainders[i]))

    def values():
        bs = []
        for i in range(count):
            update = nn(lo(inverse[i] * beta_r[i]), kvs[i][:, R:].astype(bf16))
            bs.append(tn(lo(update), remainders[i]))
        return bs

    return ns, keeps, values


def kernel(
    tok, wk, wv, wb, wd, bias_in, rate_in, finc_in, query_in, gain_in,
    packed,
    bias_ref, rate_ref, finc, query, gain,
    x, wkv, wg, acc, accg, bfull, xs, ps, zs, fs, srow,
    load_sem, rsend, rrecv, dsend, drecv, xsend, xrecv, psem, zsend, zrecv, fsend, frecv,
):
    sp = lax.axis_index("sp")
    tp = lax.axis_index("tp")
    mz, mx = sp // NX, sp % NX
    my, core = tp // 2, tp % 2
    sigma = 2 * (mz % 2) - 1

    def at_y(step):
        return {"sp": sp, "tp": ((my + step + NY) % NY) * 2 + core}

    def at_x(step):
        return {"sp": mz * NX + (mx + step) % NX, "tp": tp}

    def at_z(step):
        return {"sp": ((mz + step + NZ) % NZ) * NX + mx, "tp": tp}

    other_core = {"sp": sp, "tp": my * 2 + 1 - core}
    pair = at_z(1 - 2 * (mz % 2))

    loads = []
    for g in range(G):
        c = pltpu.make_async_copy(
            tok.at[pl.ds(g * R, R)], x.at[tp, pl.ds(g * R, R)], load_sem.at[g]
        )
        c.start()
        loads.append(c)
    weights = [
        pltpu.make_async_copy(wk, wkv.at[:, pl.ds(0, R)], load_sem.at[G]),
        pltpu.make_async_copy(wv, wkv.at[:, pl.ds(R, R)], load_sem.at[G + 1]),
        pltpu.make_async_copy(wb, wg.at[pl.ds(0, 16)], load_sem.at[G + 2]),
        pltpu.make_async_copy(wd, wg.at[pl.ds(16, 16)], load_sem.at[G + 3]),
    ]
    smalls = [
        pltpu.make_async_copy(src, dst, load_sem.at[G + 4 + i])
        for i, (src, dst) in enumerate((
            (bias_in, bias_ref), (rate_in, rate_ref), (finc_in, finc),
            (query_in, query), (gain_in, gain),
        ))
    ]

    barrier = pltpu.get_barrier_semaphore()
    peers = [at_y(1), at_y(-1), other_core, at_x(1), at_x(2), at_x(3)]
    z_peers = [at_z(sigma), at_z(3 * sigma), at_z(2 * sigma), at_z(-2 * sigma)]
    if True:
        z_peers.append(pair)
    for peer in peers + z_peers:
        pl.semaphore_signal(barrier, inc=1, device_id=peer, device_id_type=MESH)
    pl.semaphore_wait(barrier, len(peers) + len(z_peers))

    sent = []

    def shard(way, d, who):
        step = -d if way == 0 else d
        return ((my + step + NY) % NY) * 2 + who

    def rows(g):
        return pl.ds(g * R, R)

    def ring(way, d, g, sub):
        s = shard(way, d, core)
        part = x.at[s, pl.ds(g * R + sub * (R // 2), R // 2)]
        return pltpu.make_async_remote_copy(
            part, part, rsend.at[way, d, 2 * g + sub], rrecv.at[way, d, 2 * g + sub],
            device_id=at_y(1 if way == 0 else -1), device_id_type=MESH,
        )

    def landed(way, d, g, sub):
        s = shard(way, d, core)
        part = x.at[s, pl.ds(g * R + sub * (R // 2), R // 2)]
        pltpu.make_async_remote_copy(
            part, part, rsend.at[way, d - 1, 2 * g + sub], rrecv.at[way, d - 1, 2 * g + sub],
            device_id=at_y(1 if way == 0 else -1), device_id_type=MESH,
        ).wait_recv()

    def across(way, d, g):
        s = shard(way, d, core)
        c = pltpu.make_async_remote_copy(
            x.at[s, rows(g)], x.at[s, rows(g)],
            dsend.at[way, d, g], drecv.at[way, d, g],
            device_id=other_core, device_id_type=MESH,
        )
        c.start()
        sent.append(c)

    def crossed(way, d, g):
        s = shard(way, d, 1 - core)
        pltpu.make_async_remote_copy(
            x.at[s, rows(g)], x.at[s, rows(g)],
            dsend.at[way, d, g], drecv.at[way, d, g],
            device_id=other_core, device_id_type=MESH,
        ).wait_recv()

    def project(items, g, first=False):
        total, gate = None, None
        for s in items:
            piece = x[s, g * R : (g + 1) * R, :]
            at = pl.multiple_of(s * 256, 256)
            p = nn(piece, wkv[pl.ds(at, 256), :])
            q = nt(wg[:, pl.ds(at, 256)], piece)
            total = p if total is None else total + p
            gate = q if gate is None else gate + q
        if first:
            acc[g * R : (g + 1) * R, :] = total
            accg[g] = gate
        else:
            acc[g * R : (g + 1) * R, :] += total
            accg[g] += gate

    pending = []

    def take_pending(leave=0):
        while len(pending) > leave:
            way, d, g = pending.pop(0)
            crossed(way, d, g)
            project([shard(way, d, 1 - core)], g)

    def event(way, d, g, forward):
        for sub in range(2):
            landed(way, d, g, sub)
            if forward:
                c = ring(way, d, g, sub)
                c.start()
                sent.append(c)
        across(way, d, g)

    def step(d, half, leave=4):
        todo = []
        for way in range(2):
            g = half if way == 0 else half ^ 1
            event(way, d, g, d < 3 or (d == 3 and half % 2 == 0))
            todo.append((way, d, g))
        for way, d, g in todo:
            project([shard(way, d, core)], g)
            pending.append((way, d, g))
        take_pending(leave)

    def own(half):
        for way in range(2):
            g = half if way == 0 else half ^ 1
            for sub in range(2):
                c = ring(way, 0, g, sub)
                c.start()
                sent.append(c)

    loads[0].wait()
    loads[1].wait()
    own(0)
    own(1)
    across(0, 0, 0)
    across(0, 0, 1)
    for w in weights + smalls:
        w.start()
    loads[2].wait()
    loads[3].wait()
    across(0, 0, 2)
    across(0, 0, 3)
    for w in weights + smalls:
        w.wait()
    for g in range(G):
        project([tp], g, first=True)
        pending.append((0, 0, g))

    h = tp
    bias, rate = bias_ref[h], rate_ref[h]

    def blocks_of(groups):
        kvs = [acc[g * R : (g + 1) * R, :] for g in groups]
        gates = [(accg[g, pl.ds(h, 1), :], accg[g, pl.ds(16 + h, 1), :]) for g in groups]
        fincs = [finc[:, g * R : (g + 1) * R] for g in groups]
        return block_maps(kvs, gates, fincs, bias, rate)

    own(2)
    own(3)
    step(1, 0, 6)
    step(1, 1, 6)
    step(1, 2, 6)
    step(1, 3, 6)
    step(2, 0, 6)
    step(2, 1, 6)
    step(2, 2, 6)
    step(2, 3, 6)
    step(3, 0, 6)
    step(3, 1, 6)
    step(3, 2, 6)
    step(3, 3, 6)
    step(4, 0, 4)
    step(4, 2, 4)
    take_pending()
    late = None
    ns, keeps, values = blocks_of((0, 1, 2, 3))

    def n_of(n1, a1, n2, a2):
        return a2 * n1 + a1 * n2 - nn(lo(n1), lo(n2))

    n01, a01 = n_of(ns[0], keeps[0], ns[1], keeps[1]), keeps[0] * keeps[1]
    n23, a23 = n_of(ns[2], keeps[2], ns[3], keeps[3]), keeps[2] * keeps[3]
    n, a = n_of(n01, a01, n23, a23), a01 * a23

    def keep_rows(keep, qrow):
        hi = keep.astype(bf16).astype(f32)
        mid = (keep - hi).astype(bf16).astype(f32)
        rest = keep - hi - mid
        r16 = iota((16, R), 0)
        blk = jnp.where(r16 == 0, hi, jnp.where(r16 == 1, mid, jnp.where(r16 == 2, rest, 0.0)))
        return lo(jnp.where(r16 == 3, qrow, blk))

    lane1 = iota((1, R), 1)
    q4 = query[...].astype(f32)
    qrow = jnp.zeros((1, R), f32)
    for i in range(4):
        qrow = qrow + jnp.where(lane1 == 4 * sp + i, q4[:, i : i + 1], 0.0)
    xs[mx, 0:R, :] = lo(n)
    xs[mx, R : R + 16, :] = keep_rows(a, qrow)
    sent_x = []
    for o in (2, 1, 3):
        c = pltpu.make_async_remote_copy(
            xs.at[mx, pl.ds(0, R + 16)], xs.at[mx, pl.ds(0, R + 16)],
            xsend.at[0, o - 1], xrecv.at[0, o - 1], device_id=at_x(o), device_id_type=MESH,
        )
        c.start()
        sent_x.append(c)
    bs = values()

    def b_of(b1, n2, a2, b2):
        return a2 * b1 - nn(lo(b1), lo(n2)) + b2

    b01 = b_of(bs[0], ns[1], keeps[1], bs[1])
    b23 = b_of(bs[2], ns[3], keeps[3], bs[3])
    b = b_of(b01, n23, a23, b23)
    bfull[...] = lo(b).reshape(NX, 32, R)
    for o in (2, 1, 3):
        c = pltpu.make_async_remote_copy(
            bfull.at[(mx + o) % NX], xs.at[mx, pl.ds(R + 16, 32)],
            xsend.at[1, o - 1], xrecv.at[1, o - 1], device_id=at_x(o), device_id_type=MESH,
        )
        c.start()
        sent_x.append(c)
    xs[mx, R + 16 : R + 48, :] = bfull[mx]

    def unpack(ref, k):
        n_lo = ref[k, 0:R, :]
        extra = ref[k, R : R + 16, :].astype(f32)
        b_lo = ref[k, R + 16 : R + 48, :]
        keep = extra[0:1] + extra[1:2] + extra[2:3]
        nb_lo = jnp.concatenate([n_lo, b_lo], axis=0)
        return (nb_lo.astype(f32), keep, nb_lo), extra[3:4]

    for o in (1, 3, 2):
        src = (mx + NX - o) % NX
        pltpu.make_async_remote_copy(
            xs.at[src, pl.ds(0, R + 16)], xs.at[src, pl.ds(0, R + 16)],
            xsend.at[0, o - 1], xrecv.at[0, o - 1], device_id=at_x(o), device_id_type=MESH,
        ).wait_recv()
        pltpu.make_async_remote_copy(
            bfull.at[0], xs.at[src, pl.ds(R + 16, 32)],
            xsend.at[1, o - 1], xrecv.at[1, o - 1], device_id=at_x(o), device_id_type=MESH,
        ).wait_recv()
    got = [unpack(xs, k) for k in range(NX)]
    half0 = joined(*compose(got[0][0], got[1][0]))
    half1 = joined(*compose(got[2][0], got[3][0]))
    n, b, a = compose(half0, half1)
    qrow = got[0][1] + got[1][1] + got[2][1] + got[3][1]

    def put(ref, slot, n, b, a, qrow):
        ref[slot, 0:R, :] = lo(n)
        ref[slot, R : R + 16, :] = keep_rows(a, qrow)
        ref[slot, R + 16 : R + 48, :] = lo(b)

    me2 = mz % 2
    put(ps, me2, n, b, a, qrow)
    c = pltpu.make_async_remote_copy(
        ps.at[me2], ps.at[me2], psem.at[0], psem.at[1], device_id=pair, device_id_type=MESH
    )
    c.start()
    sent_x.append(c)
    pltpu.make_async_remote_copy(
        ps.at[1 - me2], ps.at[1 - me2], psem.at[0], psem.at[1], device_id=pair, device_id_type=MESH
    ).wait_recv()
    got = [unpack(ps, k) for k in range(2)]
    n, b, a = compose(got[0][0], got[1][0])
    qrow = got[0][1] + got[1][1]

    mine = mz // 2
    put(zs, mine, n, b, a, qrow)
    for o in (3, 2, 1):
        c = pltpu.make_async_remote_copy(
            zs.at[mine], zs.at[mine], zsend.at[o - 1], zrecv.at[o - 1],
            device_id=at_z(o * sigma), device_id_type=MESH,
        )
        c.start()
        sent_x.append(c)
    for o, step in ((1, 1), (2, -2), (3, 3)):
        src = ((mz + step * sigma + NZ) % NZ) // 2
        pltpu.make_async_remote_copy(
            zs.at[src], zs.at[src], zsend.at[o - 1], zrecv.at[o - 1],
            device_id=at_z(o * sigma), device_id_type=MESH,
        ).wait_recv()
    got = [unpack(zs, k) for k in range(4)]
    state = got[0][0][0][R:]
    for k in range(1, 4):
        nb, keep, nb_lo = got[k][0]
        state = keep * state - nn(lo(state), nb_lo[:R]) + nb[R:]
    qrow = got[0][1] + got[1][1] + got[2][1] + got[3][1]

    fs[mx] = lo(state)
    for o in (2, 1, 3):
        c = pltpu.make_async_remote_copy(
            fs.at[mx], fs.at[mx], fsend.at[o - 1], frecv.at[o - 1],
            device_id=at_x(o), device_id_type=MESH,
        )
        c.start()
        sent_x.append(c)
    for o in (1, 3, 2):
        src = (mx + NX - o) % NX
        pltpu.make_async_remote_copy(
            fs.at[src], fs.at[src], fsend.at[o - 1], frecv.at[o - 1],
            device_id=at_x(o), device_id_type=MESH,
        ).wait_recv()
    whole = fs[...].reshape(R, R)
    raw = nt(jnp.broadcast_to(lo(qrow), (16, R)), whole)[0:1]
    gains = gain[...].astype(f32)
    read = raw * lax.rsqrt(jnp.mean(raw * raw, axis=1, keepdims=True) + norm_eps) * gains
    srow[...] = whole.astype(f32).T
    packed[0:4, :] = srow[pl.ds(pl.multiple_of(4 * sp, 4), 4), :]
    packed[4:5, :] = read

    for c in sent + sent_x:
        c.wait_send()


def unpack_out(packed, state_out, read_out):
    state_out[0] = lo(packed[0:4, :])
    read_out[...] = packed[4:5, :]


def per_device(tokens, w_key, w_value, w_beta, w_decay, beta_bias, decay_rate, finc, query, gain):
    hbm = pl.BlockSpec(memory_space=pl.ANY)
    vmem = pl.BlockSpec(memory_space=pltpu.VMEM)
    dma = pltpu.SemaphoreType.DMA
    packed = pl.pallas_call(
        kernel,
        out_shape=pltpu.VMEM((8, R), f32),
        in_specs=[hbm] * 10,
        out_specs=vmem,
        scratch_shapes=[
            pltpu.SMEM((16,), f32),
            pltpu.SMEM((16,), f32),
            pltpu.VMEM((1, G * R), f32),
            pltpu.VMEM((1, 4), bf16),
            pltpu.VMEM((1, R), bf16),
            pltpu.VMEM((16, G * R, 256), bf16),
            pltpu.VMEM((4096, 256), bf16),
            pltpu.VMEM((32, 4096), bf16),
            pltpu.VMEM((G * R, 256), f32),
            pltpu.VMEM((G, 32, R), f32),
            pltpu.VMEM((NX, 32, R), bf16),
            pltpu.VMEM((NX, 176, R), bf16),
            pltpu.VMEM((2, 176, R), bf16),
            pltpu.VMEM((4, 176, R), bf16),
            pltpu.VMEM((NX, 32, R), bf16),
            pltpu.VMEM((R, R), f32),
            dma((G + 9,)),
            dma((2, 4, 2 * G)), dma((2, 4, 2 * G)),
            dma((2, 5, G)), dma((2, 5, G)),
            dma((2, 3)), dma((2, 3)),
            dma((2,)),
            dma((3,)), dma((3,)),
            dma((3,)), dma((3,)),
        ],
        compiler_params=pltpu.CompilerParams(
            collective_id=0, has_side_effects=True, vmem_limit_bytes=60 * 2**20
        ),
    )(
        tokens, w_key, w_value, w_beta.T, w_decay.T, beta_bias, decay_rate, finc, query,
        gain.reshape(1, R),
    )
    return pl.pallas_call(
        unpack_out,
        out_shape=(
            jax.ShapeDtypeStruct((1, 4, R), bf16),
            jax.ShapeDtypeStruct((1, R), f32),
        ),
        in_specs=[vmem],
        out_specs=(vmem, vmem),
    )(pltpu.with_memory_space_constraint(packed, pltpu.VMEM))


def solution(mesh):
    return jax.shard_map(
        per_device,
        mesh=mesh,
        in_specs=(
            P("sp", "tp"),
            P(None, "tp"),
            P(None, "tp"),
            P(),
            P(),
            P(),
            P(),
            P("tp", "sp"),
            P("tp", "sp"),
            P(),
        ),
        out_specs=(P("tp", "sp", None), P("tp", None)),
        check_vma=False,
    )
```

```python
import functools

import jax
import jax.numpy as jnp
from jax import lax
from jax.experimental import pallas as pl
from jax.experimental.pallas import tpu as pltpu
from jax.sharding import PartitionSpec as P

NX, NZ, NY = 4, 8, 8
G = 4
R = 128
MESH = pl.DeviceIdType.MESH
f32, bf16 = jnp.float32, jnp.bfloat16
norm_eps = 1e-06


def nn(a, b):
    return lax.dot_general(a, b, (((1,), (0,)), ((), ())), preferred_element_type=f32)


def nt(a, b):
    return lax.dot_general(a, b, (((1,), (1,)), ((), ())), preferred_element_type=f32)


def tn(a, b):
    return lax.dot_general(a, b, (((0,), (0,)), ((), ())), preferred_element_type=f32)


def lo(x):
    return x.astype(bf16)


def iota(shape, dim):
    return lax.broadcasted_iota(jnp.int32, shape, dim)


def compose(first, second):
    nb1, a1, nb1_lo = first
    nb2, a2, nb2_lo = second
    q = nn(nb1_lo, nb2_lo[:R])
    n = a2 * nb1[:R] + a1 * nb2[:R] - q[:R]
    b = a2 * nb1[R:] - q[R:] + nb2[R:]
    return n, b, a1 * a2


def joined(n, b, a):
    nb = jnp.concatenate([n, b], axis=0)
    return nb, a, lo(nb)


def block_maps(kvs, gates, fincs, bias, rate):
    count = len(kvs)
    row, col = iota((R, R), 0), iota((R, R), 1)
    strict = row < col
    eye = (row == col).astype(f32)
    kw = [kv[:, :R].astype(bf16) for kv in kvs]
    kw_t = [k.T for k in kw]
    kk = [nn(k, t) for k, t in zip(kw, kw_t)]
    logits = jnp.concatenate([dl for _, dl in gates] + [bl for bl, _ in gates], axis=0)
    c = -rate * jax.nn.softplus(logits) + jnp.concatenate(fincs + fincs, axis=0)
    beta = jax.nn.sigmoid(logits + bias)
    lane = iota((2 * count, R), 1)
    step = 1
    while step < R:
        c = c + jnp.where(lane >= step, pltpu.roll(c, step, 1), 0.0)
        step *= 2
    packed = jnp.where(iota((2 * count, R), 0) < count, c, beta)
    columns = packed.T
    rs, spread_rs = [], jnp.zeros((R, R), f32)
    for i, k in enumerate(kw):
        wide = k.astype(f32)
        rs.append(lax.rsqrt(jnp.sum(wide * wide, axis=1, keepdims=True) + norm_eps))
        spread_rs = jnp.where(col == i, rs[i], spread_rs)
    rs_rows = spread_rs.T
    cum_r = [packed[i : i + 1] for i in range(count)]
    cum_c = [columns[:, i : i + 1] for i in range(count)]
    beta_r = [packed[count + i : count + i + 1] for i in range(count)]
    beta_c = [columns[:, count + i : count + i + 1] for i in range(count)]
    rs_r = [rs_rows[i : i + 1] for i in range(count)]
    lower = []
    for i in range(count):
        decay = jnp.exp(jnp.where(strict, cum_r[i] - cum_c[i], 0.0))
        lower.append(jnp.where(strict, kk[i] * rs[i] * (rs_r[i] * beta_r[i]) * decay, 0.0))
    same = (row // 16) == (col // 16)
    power = [lo(jnp.where(same, l, 0.0)) for l in lower]
    inverse = [eye - jnp.where(same, l, 0.0) for l in lower]
    for _ in range(3):
        power = [lo(nn(p, p)) for p in power]
        inverse = [x + nn(lo(x), p) for x, p in zip(inverse, power)]
    size = 16
    while size < R:
        below = ((row // (2 * size)) == (col // (2 * size))) & ((row // size) < (col // size))
        short = [lo(x) for x in inverse]
        inner = [lo(nn(s, lo(jnp.where(below, l, 0.0)))) for s, l in zip(short, lower)]
        inverse = [x - nn(y, s) for x, y, s in zip(inverse, inner, short)]
        size *= 2
    ns, keeps, remainders = [], [], []
    for i in range(count):
        last = cum_r[i][:, R - 1 : R]
        keeps.append(jnp.broadcast_to(jnp.exp(last), (1, R)))
        remainders.append(lo(kw[i].astype(f32) * (rs[i] * jnp.exp(last - cum_c[i]))))
        erase_t = nn(kw_t[i], lo(inverse[i] * (beta_c[i] * jnp.exp(cum_c[i]) * rs[i])))
        ns.append(nn(lo(erase_t), remainders[i]))

    def values():
        bs = []
        for i in range(count):
            update_t = nn(kvs[i][:, R:].astype(bf16).T, lo(inverse[i] * beta_c[i]))
            bs.append(nn(lo(update_t), remainders[i]))
        return bs

    return ns, keeps, values


def kernel(
    tok, wk, wv, wb, wd, bias_in, rate_in, finc_in, query_in, gain_in,
    packed,
    bias_ref, rate_ref, finc, query, gain,
    x, wkv, wg, acc, accg, bfull, xs, ps, zs, fs, srow,
    load_sem, rsend, rrecv, dsend, drecv, xsend, xrecv, psem, zsend, zrecv, fsend, frecv,
):
    sp = lax.axis_index("sp")
    tp = lax.axis_index("tp")
    mz, mx = sp // NX, sp % NX
    my, core = tp // 2, tp % 2
    sigma = 2 * (mz % 2) - 1

    def at_y(step):
        return {"sp": sp, "tp": ((my + step + NY) % NY) * 2 + core}

    def at_x(step):
        return {"sp": mz * NX + (mx + step) % NX, "tp": tp}

    def at_z(step):
        return {"sp": ((mz + step + NZ) % NZ) * NX + mx, "tp": tp}

    other_core = {"sp": sp, "tp": my * 2 + 1 - core}
    pair = at_z(1 - 2 * (mz % 2))

    loads = []
    for g in range(G):
        c = pltpu.make_async_copy(
            tok.at[pl.ds(g * R, R)], x.at[tp, pl.ds(g * R, R)], load_sem.at[g]
        )
        c.start()
        loads.append(c)
    weights = [
        pltpu.make_async_copy(wk, wkv.at[:, pl.ds(0, R)], load_sem.at[G]),
        pltpu.make_async_copy(wv, wkv.at[:, pl.ds(R, R)], load_sem.at[G + 1]),
        pltpu.make_async_copy(wb, wg.at[pl.ds(0, 16)], load_sem.at[G + 2]),
        pltpu.make_async_copy(wd, wg.at[pl.ds(16, 16)], load_sem.at[G + 3]),
    ]
    smalls = [
        pltpu.make_async_copy(src, dst, load_sem.at[G + 4 + i])
        for i, (src, dst) in enumerate((
            (bias_in, bias_ref), (rate_in, rate_ref), (finc_in, finc),
            (query_in, query), (gain_in, gain),
        ))
    ]

    barrier = pltpu.get_barrier_semaphore()
    peers = [at_y(1), at_y(-1), other_core, at_x(1), at_x(2), at_x(3)]
    z_peers = [at_z(sigma), at_z(3 * sigma), at_z(2 * sigma), at_z(-2 * sigma)]
    if True:
        z_peers.append(pair)
    for peer in peers + z_peers:
        pl.semaphore_signal(barrier, inc=1, device_id=peer, device_id_type=MESH)
    pl.semaphore_wait(barrier, len(peers) + len(z_peers))

    sent = []

    def shard(way, d, who):
        step = -d if way == 0 else d
        return ((my + step + NY) % NY) * 2 + who

    def rows(g):
        return pl.ds(g * R, R)

    def ring(way, d, g, sub):
        s = shard(way, d, core)
        part = x.at[s, pl.ds(g * R + sub * (R // 2), R // 2)]
        return pltpu.make_async_remote_copy(
            part, part, rsend.at[way, d, 2 * g + sub], rrecv.at[way, d, 2 * g + sub],
            device_id=at_y(1 if way == 0 else -1), device_id_type=MESH,
        )

    def landed(way, d, g, sub):
        s = shard(way, d, core)
        part = x.at[s, pl.ds(g * R + sub * (R // 2), R // 2)]
        pltpu.make_async_remote_copy(
            part, part, rsend.at[way, d - 1, 2 * g + sub], rrecv.at[way, d - 1, 2 * g + sub],
            device_id=at_y(1 if way == 0 else -1), device_id_type=MESH,
        ).wait_recv()

    def across(way, d, g):
        s = shard(way, d, core)
        c = pltpu.make_async_remote_copy(
            x.at[s, rows(g)], x.at[s, rows(g)],
            dsend.at[way, d, g], drecv.at[way, d, g],
            device_id=other_core, device_id_type=MESH,
        )
        c.start()
        sent.append(c)

    def crossed(way, d, g):
        s = shard(way, d, 1 - core)
        pltpu.make_async_remote_copy(
            x.at[s, rows(g)], x.at[s, rows(g)],
            dsend.at[way, d, g], drecv.at[way, d, g],
            device_id=other_core, device_id_type=MESH,
        ).wait_recv()

    def project(items, g, first=False):
        total, gate = None, None
        for s in items:
            piece = x[s, g * R : (g + 1) * R, :]
            at = pl.multiple_of(s * 256, 256)
            p = nn(piece, wkv[pl.ds(at, 256), :])
            q = nt(wg[:, pl.ds(at, 256)], piece)
            total = p if total is None else total + p
            gate = q if gate is None else gate + q
        if first:
            acc[g * R : (g + 1) * R, :] = total
            accg[g] = gate
        else:
            acc[g * R : (g + 1) * R, :] += total
            accg[g] += gate

    pending = []

    def take_pending(leave=0):
        while len(pending) > leave:
            way, d, g = pending.pop(0)
            crossed(way, d, g)
            project([shard(way, d, 1 - core)], g)

    def event(way, d, g, forward):
        for sub in range(2):
            landed(way, d, g, sub)
            if forward:
                c = ring(way, d, g, sub)
                c.start()
                sent.append(c)
        across(way, d, g)

    def step(d, half, leave=4):
        todo = []
        for way in range(2):
            g = half if way == 0 else half ^ 1
            event(way, d, g, d < 3 or (d == 3 and half % 2 == 0))
            todo.append((way, d, g))
        for way, d, g in todo:
            project([shard(way, d, core)], g)
            pending.append((way, d, g))
        take_pending(leave)

    def own(half):
        for way in range(2):
            g = half if way == 0 else half ^ 1
            for sub in range(2):
                c = ring(way, 0, g, sub)
                c.start()
                sent.append(c)

    loads[0].wait()
    loads[1].wait()
    own(0)
    own(1)
    across(0, 0, 0)
    across(0, 0, 1)
    for w in weights + smalls:
        w.start()
    loads[2].wait()
    loads[3].wait()
    across(0, 0, 2)
    across(0, 0, 3)
    for w in weights + smalls:
        w.wait()
    for g in range(G):
        project([tp], g, first=True)
        pending.append((0, 0, g))

    h = tp
    bias, rate = bias_ref[h], rate_ref[h]

    def blocks_of(groups):
        kvs = [acc[g * R : (g + 1) * R, :] for g in groups]
        gates = [(accg[g, pl.ds(h, 1), :], accg[g, pl.ds(16 + h, 1), :]) for g in groups]
        fincs = [finc[:, g * R : (g + 1) * R] for g in groups]
        return block_maps(kvs, gates, fincs, bias, rate)

    own(2)
    own(3)
    step(1, 0, 6)
    step(1, 1, 6)
    step(1, 2, 6)
    step(1, 3, 6)
    step(2, 0, 6)
    step(2, 1, 6)
    step(2, 2, 6)
    step(2, 3, 6)
    step(3, 0, 6)
    step(3, 1, 6)
    step(3, 2, 6)
    step(3, 3, 6)
    step(4, 0, 4)
    step(4, 2, 4)
    take_pending()
    late = None
    ns, keeps, values = blocks_of((0, 1, 2, 3))

    def n_of(n1, a1, n2, a2):
        return a2 * n1 + a1 * n2 - nn(lo(n1), lo(n2))

    n01, a01 = n_of(ns[0], keeps[0], ns[1], keeps[1]), keeps[0] * keeps[1]
    n23, a23 = n_of(ns[2], keeps[2], ns[3], keeps[3]), keeps[2] * keeps[3]
    n, a = n_of(n01, a01, n23, a23), a01 * a23

    def keep_rows(keep, qrow):
        hi = keep.astype(bf16).astype(f32)
        mid = (keep - hi).astype(bf16).astype(f32)
        rest = keep - hi - mid
        r16 = iota((16, R), 0)
        blk = jnp.where(r16 == 0, hi, jnp.where(r16 == 1, mid, jnp.where(r16 == 2, rest, 0.0)))
        return lo(jnp.where(r16 == 3, qrow, blk))

    lane1 = iota((1, R), 1)
    q4 = query[...].astype(f32)
    qrow = jnp.zeros((1, R), f32)
    for i in range(4):
        qrow = qrow + jnp.where(lane1 == 4 * sp + i, q4[:, i : i + 1], 0.0)
    xs[mx, 0:R, :] = lo(n)
    xs[mx, R : R + 16, :] = keep_rows(a, qrow)
    sent_x = []
    for o in (1, 3, 2):
        c = pltpu.make_async_remote_copy(
            xs.at[mx, pl.ds(0, R + 16)], xs.at[mx, pl.ds(0, R + 16)],
            xsend.at[0, o - 1], xrecv.at[0, o - 1], device_id=at_x(o), device_id_type=MESH,
        )
        c.start()
        sent_x.append(c)
    bs = values()

    def b_of(b1, n2, a2, b2):
        return a2 * b1 - nn(lo(b1), lo(n2)) + b2

    b01 = b_of(bs[0], ns[1], keeps[1], bs[1])
    b23 = b_of(bs[2], ns[3], keeps[3], bs[3])
    b = b_of(b01, n23, a23, b23)
    bfull[...] = lo(b).reshape(NX, 32, R)
    for o in (1, 3, 2):
        c = pltpu.make_async_remote_copy(
            bfull.at[(mx + o) % NX], xs.at[mx, pl.ds(R + 16, 32)],
            xsend.at[1, o - 1], xrecv.at[1, o - 1], device_id=at_x(o), device_id_type=MESH,
        )
        c.start()
        sent_x.append(c)
    for c in sent:
        c.wait_send()
    xs[mx, R + 16 : R + 48, :] = bfull[mx]

    def unpack(ref, k):
        n_lo = ref[k, 0:R, :]
        extra = ref[k, R : R + 16, :].astype(f32)
        b_lo = ref[k, R + 16 : R + 48, :]
        keep = extra[0:1] + extra[1:2] + extra[2:3]
        nb_lo = jnp.concatenate([n_lo, b_lo], axis=0)
        return (nb_lo.astype(f32), keep, nb_lo), extra[3:4]

    for o in (1, 3, 2):
        src = (mx + NX - o) % NX
        pltpu.make_async_remote_copy(
            xs.at[src, pl.ds(0, R + 16)], xs.at[src, pl.ds(0, R + 16)],
            xsend.at[0, o - 1], xrecv.at[0, o - 1], device_id=at_x(o), device_id_type=MESH,
        ).wait_recv()
        pltpu.make_async_remote_copy(
            bfull.at[0], xs.at[src, pl.ds(R + 16, 32)],
            xsend.at[1, o - 1], xrecv.at[1, o - 1], device_id=at_x(o), device_id_type=MESH,
        ).wait_recv()
    got = [unpack(xs, k) for k in range(NX)]
    half0 = joined(*compose(got[0][0], got[1][0]))
    half1 = joined(*compose(got[2][0], got[3][0]))
    n, b, a = compose(half0, half1)
    qrow = got[0][1] + got[1][1] + got[2][1] + got[3][1]

    def put(ref, slot, n, b, a, qrow):
        ref[slot, 0:R, :] = lo(n)
        ref[slot, R : R + 16, :] = keep_rows(a, qrow)
        ref[slot, R + 16 : R + 48, :] = lo(b)

    me2 = mz % 2
    put(ps, me2, n, b, a, qrow)
    c = pltpu.make_async_remote_copy(
        ps.at[me2], ps.at[me2], psem.at[0], psem.at[1], device_id=pair, device_id_type=MESH
    )
    c.start()
    sent_x.append(c)
    pltpu.make_async_remote_copy(
        ps.at[1 - me2], ps.at[1 - me2], psem.at[0], psem.at[1], device_id=pair, device_id_type=MESH
    ).wait_recv()
    got = [unpack(ps, k) for k in range(2)]
    n, b, a = compose(got[0][0], got[1][0])
    qrow = got[0][1] + got[1][1]

    mine = mz // 2
    put(zs, mine, n, b, a, qrow)
    for o in (1, 2, 3):
        c = pltpu.make_async_remote_copy(
            zs.at[mine], zs.at[mine], zsend.at[o - 1], zrecv.at[o - 1],
            device_id=at_z(o * sigma), device_id_type=MESH,
        )
        c.start()
        sent_x.append(c)
    state, qrow = None, None
    for k in range(4):
        d = (k - mine + 4) % 4
        near = ((d + 3) // 2 + 1 - mz % 2) % 2
        index = (d % 2) * near + (1 - d % 2) * 2

        @pl.when(d != 0)
        def _():
            pltpu.make_async_remote_copy(
                zs.at[k], zs.at[k], zsend.at[index], zrecv.at[index],
                device_id=at_z(sigma), device_id_type=MESH,
            ).wait_recv()

        (nb, keep, nb_lo), q_part = unpack(zs, k)
        if k == 0:
            state, qrow = nb[R:], q_part
        else:
            state = keep * state - nn(lo(state), nb_lo[:R]) + nb[R:]
            qrow = qrow + q_part

    fs[mx] = lo(state)
    for o in (1, 3, 2):
        c = pltpu.make_async_remote_copy(
            fs.at[mx], fs.at[mx], fsend.at[o - 1], frecv.at[o - 1],
            device_id=at_x(o), device_id_type=MESH,
        )
        c.start()
        sent_x.append(c)
    for o in (1, 3, 2):
        src = (mx + NX - o) % NX
        pltpu.make_async_remote_copy(
            fs.at[src], fs.at[src], fsend.at[o - 1], frecv.at[o - 1],
            device_id=at_x(o), device_id_type=MESH,
        ).wait_recv()
    whole = fs[...].reshape(R, R)
    raw = nt(jnp.broadcast_to(lo(qrow), (16, R)), whole)[0:1]
    gains = gain[...].astype(f32)
    read = raw * lax.rsqrt(jnp.mean(raw * raw, axis=1, keepdims=True) + norm_eps) * gains
    srow[...] = whole.astype(f32).T
    packed[0:4, :] = srow[pl.ds(pl.multiple_of(4 * sp, 4), 4), :]
    packed[4:5, :] = read

    for c in sent_x:
        c.wait_send()


def unpack_out(packed, state_out, read_out):
    state_out[0] = lo(packed[0:4, :])
    read_out[...] = packed[4:5, :]


def per_device(tokens, w_key, w_value, w_beta, w_decay, beta_bias, decay_rate, finc, query, gain):
    hbm = pl.BlockSpec(memory_space=pl.ANY)
    vmem = pl.BlockSpec(memory_space=pltpu.VMEM)
    dma = pltpu.SemaphoreType.DMA
    packed = pl.pallas_call(
        kernel,
        out_shape=pltpu.VMEM((8, R), f32),
        in_specs=[hbm] * 10,
        out_specs=vmem,
        scratch_shapes=[
            pltpu.SMEM((16,), f32),
            pltpu.SMEM((16,), f32),
            pltpu.VMEM((1, G * R), f32),
            pltpu.VMEM((1, 4), bf16),
            pltpu.VMEM((1, R), bf16),
            pltpu.VMEM((16, G * R, 256), bf16),
            pltpu.VMEM((4096, 256), bf16),
            pltpu.VMEM((32, 4096), bf16),
            pltpu.VMEM((G * R, 256), f32),
            pltpu.VMEM((G, 32, R), f32),
            pltpu.VMEM((NX, 32, R), bf16),
            pltpu.VMEM((NX, 176, R), bf16),
            pltpu.VMEM((2, 176, R), bf16),
            pltpu.VMEM((4, 176, R), bf16),
            pltpu.VMEM((NX, 32, R), bf16),
            pltpu.VMEM((R, R), f32),
            dma((G + 9,)),
            dma((2, 4, 2 * G)), dma((2, 4, 2 * G)),
            dma((2, 5, G)), dma((2, 5, G)),
            dma((2, 3)), dma((2, 3)),
            dma((2,)),
            dma((3,)), dma((3,)),
            dma((3,)), dma((3,)),
        ],
        compiler_params=pltpu.CompilerParams(
            collective_id=0, has_side_effects=True, vmem_limit_bytes=60 * 2**20
        ),
    )(
        tokens, w_key, w_value, w_beta.T, w_decay.T, beta_bias, decay_rate, finc, query,
        gain.reshape(1, R),
    )
    return pl.pallas_call(
        unpack_out,
        out_shape=(
            jax.ShapeDtypeStruct((1, 4, R), bf16),
            jax.ShapeDtypeStruct((1, R), f32),
        ),
        in_specs=[vmem],
        out_specs=(vmem, vmem),
    )(pltpu.with_memory_space_constraint(packed, pltpu.VMEM))


def solution(mesh):
    return jax.shard_map(
        per_device,
        mesh=mesh,
        in_specs=(
            P("sp", "tp"),
            P(None, "tp"),
            P(None, "tp"),
            P(),
            P(),
            P(),
            P(),
            P("tp", "sp"),
            P("tp", "sp"),
            P(),
        ),
        out_specs=(P("tp", "sp", None), P("tp", None)),
        check_vma=False,
    )
```

```python
import functools

import jax
import jax.numpy as jnp
from jax import lax
from jax.experimental import pallas as pl
from jax.experimental.pallas import tpu as pltpu
from jax.sharding import PartitionSpec as P

NX, NZ, NY = 4, 8, 8
G = 4
R = 128
MESH = pl.DeviceIdType.MESH
f32, bf16 = jnp.float32, jnp.bfloat16
norm_eps = 1e-06


def nn(a, b):
    return lax.dot_general(a, b, (((1,), (0,)), ((), ())), preferred_element_type=f32)


def nt(a, b):
    return lax.dot_general(a, b, (((1,), (1,)), ((), ())), preferred_element_type=f32)


def tn(a, b):
    return lax.dot_general(a, b, (((0,), (0,)), ((), ())), preferred_element_type=f32)


def lo(x):
    return x.astype(bf16)


def iota(shape, dim):
    return lax.broadcasted_iota(jnp.int32, shape, dim)


def compose(first, second):
    nb1, a1, nb1_lo = first
    nb2, a2, nb2_lo = second
    q = nn(nb1_lo, nb2_lo[:R])
    n = a2 * nb1[:R] + a1 * nb2[:R] - q[:R]
    b = a2 * nb1[R:] - q[R:] + nb2[R:]
    return n, b, a1 * a2


def joined(n, b, a):
    nb = jnp.concatenate([n, b], axis=0)
    return nb, a, lo(nb)


def block_maps(kvs, gates, fincs, bias, rate):
    count = len(kvs)
    row, col = iota((R, R), 0), iota((R, R), 1)
    strict = row < col
    eye = (row == col).astype(f32)
    kw = [kv[:, :R].astype(bf16) for kv in kvs]
    kw_t = [k.T for k in kw]
    kk = [nn(k, t) for k, t in zip(kw, kw_t)]
    logits = jnp.concatenate([dl for _, dl in gates] + [bl for bl, _ in gates], axis=0)
    c = -rate * jax.nn.softplus(logits) + jnp.concatenate(fincs + fincs, axis=0)
    beta = jax.nn.sigmoid(logits + bias)
    lane = iota((2 * count, R), 1)
    step = 1
    while step < R:
        c = c + jnp.where(lane >= step, pltpu.roll(c, step, 1), 0.0)
        step *= 2
    packed = jnp.where(iota((2 * count, R), 0) < count, c, beta)
    columns = packed.T
    rs, spread_rs = [], jnp.zeros((R, R), f32)
    for i, k in enumerate(kw):
        wide = k.astype(f32)
        rs.append(lax.rsqrt(jnp.sum(wide * wide, axis=1, keepdims=True) + norm_eps))
        spread_rs = jnp.where(col == i, rs[i], spread_rs)
    rs_rows = spread_rs.T
    cum_r = [packed[i : i + 1] for i in range(count)]
    cum_c = [columns[:, i : i + 1] for i in range(count)]
    beta_r = [packed[count + i : count + i + 1] for i in range(count)]
    beta_c = [columns[:, count + i : count + i + 1] for i in range(count)]
    rs_r = [rs_rows[i : i + 1] for i in range(count)]
    lower = []
    for i in range(count):
        decay = jnp.exp(jnp.where(strict, cum_r[i] - cum_c[i], 0.0))
        lower.append(jnp.where(strict, kk[i] * rs[i] * (rs_r[i] * beta_r[i]) * decay, 0.0))
    same = (row // 16) == (col // 16)
    power = [lo(jnp.where(same, l, 0.0)) for l in lower]
    inverse = [eye - jnp.where(same, l, 0.0) for l in lower]
    for _ in range(3):
        power = [lo(nn(p, p)) for p in power]
        inverse = [x + nn(lo(x), p) for x, p in zip(inverse, power)]
    size = 16
    while size < R:
        below = ((row // (2 * size)) == (col // (2 * size))) & ((row // size) < (col // size))
        short = [lo(x) for x in inverse]
        inner = [lo(nn(s, lo(jnp.where(below, l, 0.0)))) for s, l in zip(short, lower)]
        inverse = [x - nn(y, s) for x, y, s in zip(inverse, inner, short)]
        size *= 2
    ns, keeps, remainders = [], [], []
    for i in range(count):
        last = cum_r[i][:, R - 1 : R]
        keeps.append(jnp.broadcast_to(jnp.exp(last), (1, R)))
        remainders.append(lo(kw[i].astype(f32) * (rs[i] * jnp.exp(last - cum_c[i]))))
        erase_t = nn(kw_t[i], lo(inverse[i] * (beta_c[i] * jnp.exp(cum_c[i]) * rs[i])))
        ns.append(nn(lo(erase_t), remainders[i]))

    def values():
        bs = []
        for i in range(count):
            update_t = nn(kvs[i][:, R:].astype(bf16).T, lo(inverse[i] * beta_c[i]))
            bs.append(nn(lo(update_t), remainders[i]))
        return bs

    return ns, keeps, values


def kernel(
    tok, wk, wv, wb, wd, bias_in, rate_in, finc_in, query_in, gain_in,
    packed,
    bias_ref, rate_ref, finc, query, gain,
    x, wkv, wg, acc, accg, bfull, xs, ps, zs, fs, srow,
    load_sem, rsend, rrecv, dsend, drecv, xsend, xrecv, psem, zsend, zrecv, fsend, frecv,
):
    sp = lax.axis_index("sp")
    tp = lax.axis_index("tp")
    mz, mx = sp // NX, sp % NX
    my, core = tp // 2, tp % 2
    sigma = 2 * (mz % 2) - 1

    def at_y(step):
        return {"sp": sp, "tp": ((my + step + NY) % NY) * 2 + core}

    def at_x(step):
        return {"sp": mz * NX + (mx + step) % NX, "tp": tp}

    def at_z(step):
        return {"sp": ((mz + step + NZ) % NZ) * NX + mx, "tp": tp}

    other_core = {"sp": sp, "tp": my * 2 + 1 - core}
    pair = at_z(1 - 2 * (mz % 2))

    loads = []
    for g in range(G):
        c = pltpu.make_async_copy(
            tok.at[pl.ds(g * R, R)], x.at[tp, pl.ds(g * R, R)], load_sem.at[g]
        )
        c.start()
        loads.append(c)
    weights = [
        pltpu.make_async_copy(wk, wkv.at[:, pl.ds(0, R)], load_sem.at[G]),
        pltpu.make_async_copy(wv, wkv.at[:, pl.ds(R, R)], load_sem.at[G + 1]),
        pltpu.make_async_copy(wb, wg.at[pl.ds(0, 16)], load_sem.at[G + 2]),
        pltpu.make_async_copy(wd, wg.at[pl.ds(16, 16)], load_sem.at[G + 3]),
    ]
    smalls = [
        pltpu.make_async_copy(src, dst, load_sem.at[G + 4 + i])
        for i, (src, dst) in enumerate((
            (bias_in, bias_ref), (rate_in, rate_ref), (finc_in, finc),
            (query_in, query), (gain_in, gain),
        ))
    ]

    barrier = pltpu.get_barrier_semaphore()
    peers = [at_y(1), at_y(-1), other_core, at_x(1), at_x(2), at_x(3)]
    z_peers = [at_z(sigma), at_z(3 * sigma), at_z(2 * sigma), at_z(-2 * sigma)]
    if True:
        z_peers.append(pair)
    for peer in peers + z_peers:
        pl.semaphore_signal(barrier, inc=1, device_id=peer, device_id_type=MESH)
    pl.semaphore_wait(barrier, len(peers) + len(z_peers))

    sent = []

    def shard(way, d, who):
        step = -d if way == 0 else d
        return ((my + step + NY) % NY) * 2 + who

    def rows(g):
        return pl.ds(g * R, R)

    def ring(way, d, g, sub):
        s = shard(way, d, core)
        part = x.at[s, pl.ds(g * R + sub * (R // 2), R // 2)]
        return pltpu.make_async_remote_copy(
            part, part, rsend.at[way, d, 2 * g + sub], rrecv.at[way, d, 2 * g + sub],
            device_id=at_y(1 if way == 0 else -1), device_id_type=MESH,
        )

    def landed(way, d, g, sub):
        s = shard(way, d, core)
        part = x.at[s, pl.ds(g * R + sub * (R // 2), R // 2)]
        pltpu.make_async_remote_copy(
            part, part, rsend.at[way, d - 1, 2 * g + sub], rrecv.at[way, d - 1, 2 * g + sub],
            device_id=at_y(1 if way == 0 else -1), device_id_type=MESH,
        ).wait_recv()

    def across(way, d, g):
        s = shard(way, d, core)
        c = pltpu.make_async_remote_copy(
            x.at[s, rows(g)], x.at[s, rows(g)],
            dsend.at[way, d, g], drecv.at[way, d, g],
            device_id=other_core, device_id_type=MESH,
        )
        c.start()
        sent.append(c)

    def crossed(way, d, g):
        s = shard(way, d, 1 - core)
        pltpu.make_async_remote_copy(
            x.at[s, rows(g)], x.at[s, rows(g)],
            dsend.at[way, d, g], drecv.at[way, d, g],
            device_id=other_core, device_id_type=MESH,
        ).wait_recv()

    def project(items, g, first=False):
        total, gate = None, None
        for s in items:
            piece = x[s, g * R : (g + 1) * R, :]
            at = pl.multiple_of(s * 256, 256)
            p = nn(piece, wkv[pl.ds(at, 256), :])
            q = nt(wg[:, pl.ds(at, 256)], piece)
            total = p if total is None else total + p
            gate = q if gate is None else gate + q
        if first:
            acc[g * R : (g + 1) * R, :] = total
            accg[g] = gate
        else:
            acc[g * R : (g + 1) * R, :] += total
            accg[g] += gate

    pending = []

    def take_pending(leave=0):
        while len(pending) > leave:
            way, d, g = pending.pop(0)
            crossed(way, d, g)
            project([shard(way, d, 1 - core)], g)

    def event(way, d, g, forward):
        for sub in range(2):
            landed(way, d, g, sub)
            if forward:
                c = ring(way, d, g, sub)
                c.start()
                sent.append(c)
        across(way, d, g)

    def step(d, half, leave=4):
        todo = []
        for way in range(2):
            g = half if way == 0 else half ^ 1
            event(way, d, g, d < 3 or (d == 3 and half % 2 == 0))
            todo.append((way, d, g))
        for way, d, g in todo:
            project([shard(way, d, core)], g)
            pending.append((way, d, g))
        take_pending(leave)

    def own(half):
        for way in range(2):
            g = half if way == 0 else half ^ 1
            for sub in range(2):
                c = ring(way, 0, g, sub)
                c.start()
                sent.append(c)

    loads[0].wait()
    loads[1].wait()
    own(0)
    own(1)
    across(0, 0, 0)
    across(0, 0, 1)
    for w in weights + smalls:
        w.start()
    loads[2].wait()
    loads[3].wait()
    across(0, 0, 2)
    across(0, 0, 3)
    for w in weights + smalls:
        w.wait()
    for g in range(G):
        project([tp], g, first=True)
        pending.append((0, 0, g))

    h = tp
    bias, rate = bias_ref[h], rate_ref[h]

    def blocks_of(groups):
        kvs = [acc[g * R : (g + 1) * R, :] for g in groups]
        gates = [(accg[g, pl.ds(h, 1), :], accg[g, pl.ds(16 + h, 1), :]) for g in groups]
        fincs = [finc[:, g * R : (g + 1) * R] for g in groups]
        return block_maps(kvs, gates, fincs, bias, rate)

    own(2)
    own(3)
    step(1, 0, 6)
    step(1, 1, 6)
    step(1, 2, 6)
    step(1, 3, 6)
    step(2, 0, 6)
    step(2, 1, 6)
    step(2, 2, 6)
    step(2, 3, 6)
    step(3, 0, 6)
    step(3, 1, 6)
    step(3, 2, 6)
    step(3, 3, 6)
    step(4, 0, 4)
    step(4, 2, 4)
    take_pending()
    late = None
    ns, keeps, values = blocks_of((0, 1, 2, 3))

    def n_of(n1, a1, n2, a2):
        return a2 * n1 + a1 * n2 - nn(lo(n1), lo(n2))

    n01, a01 = n_of(ns[0], keeps[0], ns[1], keeps[1]), keeps[0] * keeps[1]
    n23, a23 = n_of(ns[2], keeps[2], ns[3], keeps[3]), keeps[2] * keeps[3]
    n, a = n_of(n01, a01, n23, a23), a01 * a23

    def keep_rows(keep, qrow):
        hi = keep.astype(bf16).astype(f32)
        mid = (keep - hi).astype(bf16).astype(f32)
        rest = keep - hi - mid
        r16 = iota((16, R), 0)
        blk = jnp.where(r16 == 0, hi, jnp.where(r16 == 1, mid, jnp.where(r16 == 2, rest, 0.0)))
        return lo(jnp.where(r16 == 3, qrow, blk))

    lane1 = iota((1, R), 1)
    q4 = query[...].astype(f32)
    qrow = jnp.zeros((1, R), f32)
    for i in range(4):
        qrow = qrow + jnp.where(lane1 == 4 * sp + i, q4[:, i : i + 1], 0.0)
    xs[mx, 0:R, :] = lo(n)
    xs[mx, R : R + 16, :] = keep_rows(a, qrow)
    sent_x = []
    for o in (1, 3, 2):
        c = pltpu.make_async_remote_copy(
            xs.at[mx, pl.ds(0, R + 16)], xs.at[mx, pl.ds(0, R + 16)],
            xsend.at[0, o - 1], xrecv.at[0, o - 1], device_id=at_x(o), device_id_type=MESH,
        )
        c.start()
        sent_x.append(c)
    bs = values()

    def b_of(b1, n2, a2, b2):
        return a2 * b1 - nn(lo(b1), lo(n2)) + b2

    b01 = b_of(bs[0], ns[1], keeps[1], bs[1])
    b23 = b_of(bs[2], ns[3], keeps[3], bs[3])
    b = b_of(b01, n23, a23, b23)
    bfull[...] = lo(b).reshape(NX, 32, R)
    for o in (1, 3, 2):
        c = pltpu.make_async_remote_copy(
            bfull.at[(mx + o) % NX], xs.at[mx, pl.ds(R + 16, 32)],
            xsend.at[1, o - 1], xrecv.at[1, o - 1], device_id=at_x(o), device_id_type=MESH,
        )
        c.start()
        sent_x.append(c)
    for c in sent:
        c.wait_send()
    xs[mx, R + 16 : R + 48, :] = bfull[mx]

    def unpack(ref, k):
        n_lo = ref[k, 0:R, :]
        extra = ref[k, R : R + 16, :].astype(f32)
        b_lo = ref[k, R + 16 : R + 48, :]
        keep = extra[0:1] + extra[1:2] + extra[2:3]
        nb_lo = jnp.concatenate([n_lo, b_lo], axis=0)
        return (nb_lo.astype(f32), keep, nb_lo), extra[3:4]

    for o in (1, 3, 2):
        src = (mx + NX - o) % NX
        pltpu.make_async_remote_copy(
            xs.at[src, pl.ds(0, R + 16)], xs.at[src, pl.ds(0, R + 16)],
            xsend.at[0, o - 1], xrecv.at[0, o - 1], device_id=at_x(o), device_id_type=MESH,
        ).wait_recv()
        pltpu.make_async_remote_copy(
            bfull.at[0], xs.at[src, pl.ds(R + 16, 32)],
            xsend.at[1, o - 1], xrecv.at[1, o - 1], device_id=at_x(o), device_id_type=MESH,
        ).wait_recv()
    got = [unpack(xs, k) for k in range(NX)]
    half0 = joined(*compose(got[0][0], got[1][0]))
    half1 = joined(*compose(got[2][0], got[3][0]))
    n, b, a = compose(half0, half1)
    qrow = got[0][1] + got[1][1] + got[2][1] + got[3][1]

    def put(ref, slot, n, b, a, qrow):
        ref[slot, 0:R, :] = lo(n)
        ref[slot, R : R + 16, :] = keep_rows(a, qrow)
        ref[slot, R + 16 : R + 48, :] = lo(b)

    me2 = mz % 2
    put(ps, me2, n, b, a, qrow)
    c = pltpu.make_async_remote_copy(
        ps.at[me2], ps.at[me2], psem.at[0], psem.at[1], device_id=pair, device_id_type=MESH
    )
    c.start()
    sent_x.append(c)
    pltpu.make_async_remote_copy(
        ps.at[1 - me2], ps.at[1 - me2], psem.at[0], psem.at[1], device_id=pair, device_id_type=MESH
    ).wait_recv()
    got = [unpack(ps, k) for k in range(2)]
    n, b, a = compose(got[0][0], got[1][0])
    qrow = got[0][1] + got[1][1]

    mine = mz // 2
    put(zs, mine, n, b, a, qrow)
    for o in (1, 2, 3):
        c = pltpu.make_async_remote_copy(
            zs.at[mine], zs.at[mine], zsend.at[o - 1], zrecv.at[o - 1],
            device_id=at_z(o * sigma), device_id_type=MESH,
        )
        c.start()
        sent_x.append(c)
    state, qrow = None, None
    for k in range(4):
        d = (k - mine + 4) % 4
        near = ((d + 3) // 2 + 1 - mz % 2) % 2
        index = (d % 2) * near + (1 - d % 2) * 2

        @pl.when(d != 0)
        def _():
            pltpu.make_async_remote_copy(
                zs.at[k], zs.at[k], zsend.at[index], zrecv.at[index],
                device_id=at_z(sigma), device_id_type=MESH,
            ).wait_recv()

        (nb, keep, nb_lo), q_part = unpack(zs, k)
        if k == 0:
            state, qrow = nb[R:], q_part
        else:
            state = keep * state - nn(lo(state), nb_lo[:R]) + nb[R:]
            qrow = qrow + q_part

    fs[mx] = lo(state)
    for o in (1, 3, 2):
        c = pltpu.make_async_remote_copy(
            fs.at[mx], fs.at[mx], fsend.at[o - 1], frecv.at[o - 1],
            device_id=at_x(o), device_id_type=MESH,
        )
        c.start()
        sent_x.append(c)
    for o in (1, 3, 2):
        src = (mx + NX - o) % NX
        pltpu.make_async_remote_copy(
            fs.at[src], fs.at[src], fsend.at[o - 1], frecv.at[o - 1],
            device_id=at_x(o), device_id_type=MESH,
        ).wait_recv()
    whole = fs[...].reshape(R, R)
    raw = nt(jnp.broadcast_to(lo(qrow), (16, R)), whole)[0:1]
    gains = gain[...].astype(f32)
    read = raw * lax.rsqrt(jnp.mean(raw * raw, axis=1, keepdims=True) + norm_eps) * gains
    srow[...] = whole.astype(f32).T
    packed[0:4, :] = srow[pl.ds(pl.multiple_of(4 * sp, 4), 4), :]
    packed[4:5, :] = read

    for c in sent_x:
        c.wait_send()


def unpack_out(packed, state_out, read_out, state, read, sem):
    read[...] = packed[4:5, :]
    state[0] = lo(packed[0:4, :])
    copies = [
        pltpu.make_async_copy(state, state_out, sem.at[0]),
        pltpu.make_async_copy(read, read_out, sem.at[1]),
    ]
    for c in copies:
        c.start()
    for c in copies:
        c.wait()


def per_device(tokens, w_key, w_value, w_beta, w_decay, beta_bias, decay_rate, finc, query, gain):
    hbm = pl.BlockSpec(memory_space=pl.ANY)
    vmem = pl.BlockSpec(memory_space=pltpu.VMEM)
    dma = pltpu.SemaphoreType.DMA
    packed = pl.pallas_call(
        kernel,
        out_shape=pltpu.VMEM((8, R), f32),
        in_specs=[hbm] * 10,
        out_specs=vmem,
        scratch_shapes=[
            pltpu.SMEM((16,), f32),
            pltpu.SMEM((16,), f32),
            pltpu.VMEM((1, G * R), f32),
            pltpu.VMEM((1, 4), bf16),
            pltpu.VMEM((1, R), bf16),
            pltpu.VMEM((16, G * R, 256), bf16),
            pltpu.VMEM((4096, 256), bf16),
            pltpu.VMEM((32, 4096), bf16),
            pltpu.VMEM((G * R, 256), f32),
            pltpu.VMEM((G, 32, R), f32),
            pltpu.VMEM((NX, 32, R), bf16),
            pltpu.VMEM((NX, 176, R), bf16),
            pltpu.VMEM((2, 176, R), bf16),
            pltpu.VMEM((4, 176, R), bf16),
            pltpu.VMEM((NX, 32, R), bf16),
            pltpu.VMEM((R, R), f32),
            dma((G + 9,)),
            dma((2, 4, 2 * G)), dma((2, 4, 2 * G)),
            dma((2, 5, G)), dma((2, 5, G)),
            dma((2, 3)), dma((2, 3)),
            dma((2,)),
            dma((3,)), dma((3,)),
            dma((3,)), dma((3,)),
        ],
        compiler_params=pltpu.CompilerParams(
            collective_id=0, has_side_effects=True, vmem_limit_bytes=60 * 2**20,
        ),
    )(
        tokens, w_key, w_value, w_beta.T, w_decay.T, beta_bias, decay_rate, finc, query,
        gain.reshape(1, R),
    )
    return pl.pallas_call(
        unpack_out,
        out_shape=(
            jax.ShapeDtypeStruct((1, 4, R), bf16),
            jax.ShapeDtypeStruct((1, R), f32),
        ),
        in_specs=[vmem],
        out_specs=(hbm, hbm),
        scratch_shapes=[pltpu.VMEM((1, 4, R), bf16), pltpu.VMEM((1, R), f32), dma((2,))],
    )(pltpu.with_memory_space_constraint(packed, pltpu.VMEM))


def solution(mesh):
    return jax.shard_map(
        per_device,
        mesh=mesh,
        in_specs=(
            P("sp", "tp"),
            P(None, "tp"),
            P(None, "tp"),
            P(),
            P(),
            P(),
            P(),
            P("tp", "sp"),
            P("tp", "sp"),
            P(),
        ),
        out_specs=(P("tp", "sp", None), P("tp", None)),
        check_vma=False,
    )
```
